32 devices in a mesh: kv: 8 (over z, y), tp: 4 (over x, core).
Axes of the slice: x: 2, y: 2, z: 4, core: 2. Of those that a mesh axis runs over, the one named last changes fastest.
Arguments:
- hidden_rows: bfloat16 [8192, 4096], P(('kv', 'tp')), may hold values from -6 to 6
- queries: bfloat16 [8192, 4096], P('kv', 'tp'), may hold values from -6 to 6
- key_rows: bfloat16 [8192, 1024], P('kv', 'tp'), may hold values from -6 to 6
- value_rows: bfloat16 [8192, 1024], P('kv', 'tp'), may hold values from -6 to 6
- branch_gates: float32 [2, 32, 8192], P(None, 'tp', 'kv'), may hold values from 0.05 to 0.95
- log_sums: float32 [2, 32, 8192], P(None, 'tp', 'kv'), may hold values from 1 to 7
- chosen: int32 [8, 64, 16], P('tp', 'kv'), may hold values from 0 to 255, as said below
- out_grad: bfloat16 [8192, 4096], P('kv', 'tp'), may hold values from -6 to 6
Outputs:
- grad_queries: bfloat16 [8192, 4096], P('kv', 'tp')
- grad_keys: bfloat16 [8192, 1024], P('kv', 'tp')
- grad_values: bfloat16 [8192, 1024], P('kv', 'tp')
- grad_weight: float32 [4096, 4096], P('kv', 'tp')
The draws below stay inside these ranges and needn't reach their ends.
Inputs may be any that keep to these rules, and one draw needn't show every extreme that they name: `chosen`: each list names distinct key blocks, among them the blocks that cover the query block's own rows; blocks past a query's position may be named and carry no weight for it. For one key head, the lists of the query blocks of one index of kv name at most 16 key blocks (counted with repetition) that lie at any one other index of kv.
All inputs are finite; a program needn't handle non-finite values.
Results may differ from the reference program's by a relative error of at most 0.011.
Values may be sent and summed in bfloat16 or wider, within the bound.
A program may use at most 128 MiB of HBM per device.

```python
import jax
import jax.numpy as jnp
from jax import lax

MODEL = 4096
HEADS = 32
KV_HEADS = 8
HEAD_DIM = 128
TOK_DEV = 1024
QUERY_BLOCK = 128
KEY_BLOCK = 32
POOL_BLOCK = 32
CHOSEN = 16
SEQ = 8192


def block_shared_rows(key):
    width = KV_HEADS * HEAD_DIM
    pool_count = SEQ // POOL_BLOCK
    key_parts = jax.random.split(key, 2)
    common = 0.8 * jax.random.normal(key_parts[0], (pool_count, 1, width), jnp.float32)
    rough = 0.6 * jax.random.normal(key_parts[1], (pool_count, POOL_BLOCK, width), jnp.float32)
    rows = jnp.clip((common + rough).reshape(SEQ, width), -6.0, 6.0)
    return rows.astype(jnp.bfloat16)


def draw_key_rows(key, part):
    return block_shared_rows(jax.random.fold_in(key, 31))


def draw_value_rows(key, part):
    return block_shared_rows(jax.random.fold_in(key, 37))


def draw_log_sums(key, part):
    key_parts = jax.random.split(jax.random.fold_in(key, 17), 2)
    seen_count = (jnp.arange(SEQ, dtype=jnp.int32) + 1) // POOL_BLOCK
    pool_level = jnp.log((seen_count + 3).astype(jnp.float32))[None, None, :]
    pooled_part = jnp.minimum(pool_level + jax.random.uniform(key_parts[0], (1, HEADS, SEQ), jnp.float32, 0.25, 0.75), 7.0)
    chosen_part = jax.random.uniform(key_parts[1], (1, HEADS, SEQ), jnp.float32, 5.0, 7.0)
    return jnp.concatenate([pooled_part, chosen_part], axis=0).astype(jnp.float32)


def draw_chosen(key, part):
    devices = SEQ // TOK_DEV
    per_device = TOK_DEV // QUERY_BLOCK
    blocks_here = TOK_DEV // KEY_BLOCK
    own_count = QUERY_BLOCK // KEY_BLOCK
    query_blocks = SEQ // QUERY_BLOCK
    free_owners = (CHOSEN - own_count) // 2 - 2
    pair_count = free_owners + 2
    key_parts = jax.random.split(key, 6)
    block_ids = jnp.arange(query_blocks, dtype=jnp.int32)
    device_of = block_ids // per_device
    owner_ids = jnp.arange(devices, dtype=jnp.int32)
    before = (device_of - 1) % devices
    across = (device_of + devices // 2) % devices
    hot_owner = jax.random.randint(key_parts[0], (KV_HEADS, 1, 1), 0, devices)
    owner_score = jax.random.randint(key_parts[1], (KV_HEADS, query_blocks, devices), 0, 1000)
    owner_score = owner_score + jnp.where(owner_ids[None, None, :] == hot_owner, 2000, 0)
    banned = (owner_ids[None, :] == device_of[:, None]) | (owner_ids[None, :] == before[:, None]) | (owner_ids[None, :] == across[:, None])
    owner_score = jnp.where(banned[None], -1, owner_score) * devices + owner_ids[None, None, :]
    _, drawn_owners = lax.top_k(owner_score, free_owners)
    fixed_owners = jnp.broadcast_to(jnp.stack([before, across], axis=-1)[None], (KV_HEADS, query_blocks, 2))
    pair_owners = jnp.concatenate([fixed_owners, drawn_owners.astype(jnp.int32)], axis=-1)
    shape = (KV_HEADS, query_blocks, pair_count)
    first_pick = jnp.minimum(jax.random.randint(key_parts[2], shape, 0, blocks_here), jax.random.randint(key_parts[3], shape, 0, blocks_here))
    second_pick = (first_pick + 1 + jax.random.randint(key_parts[4], shape, 0, blocks_here - 1)) % blocks_here
    others = jnp.concatenate([pair_owners * blocks_here + first_pick, pair_owners * blocks_here + second_pick], axis=-1)
    own_blocks = block_ids[:, None] * own_count + jnp.arange(own_count, dtype=jnp.int32)[None, :]
    own_blocks = jnp.broadcast_to(own_blocks[None], (KV_HEADS, query_blocks, own_count))
    block_lists = jnp.concatenate([own_blocks, others], axis=-1).astype(jnp.int32)
    sort_keys = jax.random.randint(key_parts[5], (KV_HEADS, query_blocks, CHOSEN), 0, 1 << 20) * CHOSEN + jnp.arange(CHOSEN, dtype=jnp.int32)
    reorder = jnp.argsort(sort_keys, axis=-1)
    return jnp.take_along_axis(block_lists, reorder, axis=-1).astype(jnp.int32)


def levels(rng, extent, shards, low, largest):
    def one(dim, blocks):
        steps = jax.random.uniform(jax.random.fold_in(jax.random.fold_in(rng, 6), dim), (blocks,), jnp.float32, low / len(shards), largest / len(shards))
        return jnp.repeat(jnp.exp(steps), extent[dim] // blocks).reshape((-1,) + (1,) * (len(extent) - dim - 1))

    factor_of = one(*shards[0])
    for cut in shards[1:]:
        factor_of = factor_of * one(*cut)
    return factor_of


def scatter_about(key, shape, deviation, reach, cuts=(), held_as=jnp.bfloat16):
    entries = deviation * jax.random.normal(key, shape, jnp.float32)
    if cuts:
        entries = entries * levels(key, shape, cuts, -0.22, 0.18)
    return jnp.clip(entries, -reach, reach).astype(held_as)


def setup_inputs(seed: int = 0) -> dict:
    arg_keys = jax.random.split(jax.random.key(seed), 9)
    return {
        "hidden_rows": scatter_about(arg_keys[0], (SEQ, MODEL), 1.0, 6.0, ((0, 32),)),
        "queries": scatter_about(arg_keys[1], (SEQ, HEADS * HEAD_DIM), 1.0, 6.0, ((0, 8), (1, 4))),
        "key_rows": draw_key_rows(jax.random.fold_in(arg_keys[8], 71), 0),
        "value_rows": draw_value_rows(jax.random.fold_in(arg_keys[8], 71), 0),
        "branch_gates": jnp.clip(0.05 + 0.9 * jax.random.uniform(arg_keys[4], (2, HEADS, SEQ), jnp.float32) ** levels(arg_keys[4], (2, HEADS, SEQ), ((1, 4), (2, 8)), -0.2, 0.2), 0.05, 0.95),
        "log_sums": draw_log_sums(jax.random.fold_in(arg_keys[8], 71), 0),
        "chosen": draw_chosen(jax.random.fold_in(arg_keys[8], 71), 0),
        "out_grad": scatter_about(arg_keys[7], (SEQ, HEADS * HEAD_DIM), 1.0, 6.0, ((0, 8), (1, 4))),
    }


def rounded(value):
    return lax.optimization_barrier(value.astype(jnp.bfloat16)).astype(jnp.float32)


def attend_back(query_rows, key_set, value_set, cotangent, log_sum, visible, score_scale):
    query_wide = query_rows.astype(jnp.float32)
    key_wide = key_set.astype(jnp.float32)
    value_wide = value_set.astype(jnp.float32)
    scores = jnp.einsum('grd,md->grm', query_wide, key_wide) * score_scale
    weights = jnp.where(visible[None], jnp.exp(scores - log_sum[:, :, None]), 0.0)
    weights_low = rounded(weights)
    branch_out = jnp.einsum('grm,md->grd', weights_low, value_wide)
    row_delta = jnp.sum(cotangent * branch_out, axis=-1)
    grad_prob = jnp.einsum('grd,md->grm', cotangent, value_wide)
    dscore = rounded(weights * (grad_prob - row_delta[:, :, None]))
    dquery = jnp.einsum('grm,md->grd', dscore, key_wide) * score_scale
    grad_key = jnp.einsum('grm,grd->md', dscore, query_wide) * score_scale
    grad_value = jnp.einsum('grm,grd->md', weights_low, cotangent)
    return dquery, grad_key, grad_value


def reference(hidden_rows, queries, key_rows, value_rows, branch_gates, log_sums, chosen, out_grad):
    seq_len = queries.shape[0]
    group_size = HEADS // KV_HEADS
    score_scale = HEAD_DIM ** -0.5
    pool_count = seq_len // POOL_BLOCK
    query_blocks = seq_len // QUERY_BLOCK
    positions = jnp.arange(seq_len, dtype=jnp.int32)
    pool_end = jnp.arange(pool_count, dtype=jnp.int32) * POOL_BLOCK + POOL_BLOCK - 1
    pool_visible = pool_end[None, :] <= positions[:, None]
    block_offsets = jnp.arange(KEY_BLOCK, dtype=jnp.int32)
    query_offsets = jnp.arange(QUERY_BLOCK, dtype=jnp.int32)

    def per_head(which_head):
        key_cols = lax.dynamic_slice_in_dim(key_rows, which_head * HEAD_DIM, HEAD_DIM, 1)
        value_cols = lax.dynamic_slice_in_dim(value_rows, which_head * HEAD_DIM, HEAD_DIM, 1)
        first_col = which_head * group_size * HEAD_DIM
        query_cols = lax.dynamic_slice_in_dim(queries, first_col, group_size * HEAD_DIM, 1)
        query_cols = query_cols.reshape(seq_len, group_size, HEAD_DIM).transpose(1, 0, 2)
        grad_cols = lax.dynamic_slice_in_dim(out_grad, first_col, group_size * HEAD_DIM, 1)
        grad_cols = grad_cols.reshape(seq_len, group_size, HEAD_DIM).transpose(1, 0, 2).astype(jnp.float32)
        gate_cols = lax.dynamic_slice_in_dim(branch_gates, which_head * group_size, group_size, 1)
        sum_cols = lax.dynamic_slice_in_dim(log_sums, which_head * group_size, group_size, 1)
        pooled_keys = jnp.mean(key_cols.astype(jnp.float32).reshape(pool_count, POOL_BLOCK, HEAD_DIM), axis=1).astype(jnp.bfloat16)
        pooled_values = jnp.mean(value_cols.astype(jnp.float32).reshape(pool_count, POOL_BLOCK, HEAD_DIM), axis=1).astype(jnp.bfloat16)
        cot_pool = rounded(gate_cols[0][:, :, None] * grad_cols)
        cot_chosen = rounded(gate_cols[1][:, :, None] * grad_cols)
        pool_dquery, pool_dkeys, pool_dvalues = attend_back(query_cols, pooled_keys, pooled_values, cot_pool, sum_cols[0], pool_visible, score_scale)
        head_lists = lax.dynamic_index_in_dim(chosen, which_head, 0, keepdims=False)

        def one_block(totals, block_index):
            key_total, value_total = totals
            picked = lax.dynamic_index_in_dim(head_lists, block_index, 0, keepdims=False)
            key_index = (picked[:, None] * KEY_BLOCK + block_offsets[None, :]).reshape(-1).astype(jnp.int32)
            row_start = (block_index * QUERY_BLOCK).astype(jnp.int32)
            query_part = lax.dynamic_slice_in_dim(query_cols, row_start, QUERY_BLOCK, 1)
            cot_part = lax.dynamic_slice_in_dim(cot_chosen, row_start, QUERY_BLOCK, 1)
            sum_part = lax.dynamic_slice_in_dim(sum_cols[1], row_start, QUERY_BLOCK, 1)
            visible = key_index[None, :] <= (row_start + query_offsets)[:, None]
            dquery, grad_key, grad_value = attend_back(query_part, key_cols[key_index], value_cols[key_index], cot_part, sum_part, visible, score_scale)
            return (key_total.at[key_index].add(grad_key), value_total.at[key_index].add(grad_value)), dquery

        empty_rows = jnp.zeros((seq_len, HEAD_DIM), jnp.float32)
        (pick_dkeys, pick_dvalues), pick_dquery = lax.scan(one_block, (empty_rows, empty_rows), jnp.arange(query_blocks, dtype=jnp.int32))
        pick_dquery = pick_dquery.transpose(1, 0, 2, 3).reshape(group_size, seq_len, HEAD_DIM)
        head_query = (pool_dquery + pick_dquery).astype(jnp.bfloat16).transpose(1, 0, 2).reshape(seq_len, group_size * HEAD_DIM)
        head_key = (pick_dkeys + jnp.repeat(pool_dkeys, POOL_BLOCK, axis=0) / POOL_BLOCK).astype(jnp.bfloat16)
        head_value = (pick_dvalues + jnp.repeat(pool_dvalues, POOL_BLOCK, axis=0) / POOL_BLOCK).astype(jnp.bfloat16)
        return head_query, head_key, head_value

    head_queries, head_keys, head_values = lax.map(per_head, jnp.arange(KV_HEADS, dtype=jnp.int32))
    grad_queries = head_queries.transpose(1, 0, 2).reshape(seq_len, HEADS * HEAD_DIM)
    grad_keys = head_keys.transpose(1, 0, 2).reshape(seq_len, KV_HEADS * HEAD_DIM)
    grad_values = head_values.transpose(1, 0, 2).reshape(seq_len, KV_HEADS * HEAD_DIM)
    grad_weight = jnp.dot(hidden_rows.T, grad_queries, preferred_element_type=jnp.float32)
    return grad_queries, grad_keys, grad_values, grad_weight
```

```python
import functools

import jax
import jax.numpy as jnp
from jax import lax
from jax.experimental import pallas as pl
from jax.experimental.pallas import tpu as pltpu
from jax.sharding import PartitionSpec as P

HEADS = 32
KV_HEADS = 8
HEAD_DIM = 128
QUERY_BLOCK = 128
KEY_BLOCK = 32
POOL_BLOCK = 32
CHOSEN = 16
CAP = 16

F32 = jnp.float32
BF16 = jnp.bfloat16
MESH = pl.DeviceIdType.MESH
VMEM_LIMIT = 62 * 2**20


def dot_nt(a, b):
    return lax.dot_general(a, b, (((1,), (1,)), ((), ())), preferred_element_type=F32)


def dot_nn(a, b):
    return lax.dot_general(a, b, (((1,), (0,)), ((), ())), preferred_element_type=F32)


def branch_back(keys, values, query_stack, cot_stack, log_row, mask, scale):
    scores = dot_nt(keys, query_stack) * scale
    weights = jnp.where(mask, jnp.exp(scores - log_row), 0.0)
    weights_low = weights.astype(BF16)
    grad_prob = dot_nt(values, cot_stack)
    delta = jnp.sum(weights_low.astype(F32) * grad_prob, axis=0, keepdims=True)
    dscore = (weights * (grad_prob - delta)).astype(BF16)
    dquery = dot_nn(keys.T, dscore)
    return dquery, dot_nn(dscore, query_stack) * scale, dot_nn(weights_low, cot_stack)


def attend_kernel(
    group, section, kv_count, scale,
    place_ref, lists_ref, slot_ref, own_ref,
    q_ref, g_ref, gate_ref, log_ref, k_ref, v_ref,
    dq_ref, send_ref, kept_ref,
    pooled_k, pooled_v, pool_dk, pool_dv, kept,
):
    head = pl.program_id(0)
    step = pl.program_id(1)
    pool_count = pooled_k.shape[0]
    tokens = kept_ref.shape[0]
    pool_here = pool_count // kv_count
    chunk = 8 * POOL_BLOCK

    @pl.when(step == 0)
    def _():
        send_ref[...] = jnp.zeros_like(send_ref)
        kept[...] = jnp.zeros_like(kept)
        pool_dk[...] = jnp.zeros_like(pool_dk)
        pool_dv[...] = jnp.zeros_like(pool_dv)
        pick = (
            lax.broadcasted_iota(jnp.int32, (16, 2 * chunk), 1) // POOL_BLOCK
            == lax.broadcasted_iota(jnp.int32, (16, 2 * chunk), 0)
        ).astype(BF16)

        def pool(i, carry):
            rows = pl.ds(pl.multiple_of(i * 2 * chunk, 2 * chunk), 2 * chunk)
            dest = pl.ds(pl.multiple_of(i * 16, 16), 16)
            pooled_k[dest, :] = (dot_nn(pick, k_ref[rows, :]) / POOL_BLOCK).astype(BF16)
            pooled_v[dest, :] = (dot_nn(pick, v_ref[rows, :]) / POOL_BLOCK).astype(BF16)
            return carry

        lax.fori_loop(0, pool_count // 16, pool, 0)

    query_stack = jnp.concatenate(
        [q_ref[:, r * HEAD_DIM : (r + 1) * HEAD_DIM] for r in range(group)], axis=0
    )
    gates = gate_ref[0].T
    grads = [g_ref[:, r * HEAD_DIM : (r + 1) * HEAD_DIM].astype(F32) for r in range(group)]

    def gated(branch):
        cols = [gates[:, branch * group + r : branch * group + r + 1] for r in range(group)]
        return jnp.concatenate([(c * g).astype(BF16) for c, g in zip(cols, grads)], axis=0)

    def log_row(branch):
        return jnp.concatenate(
            [log_ref[0, branch * group + r : branch * group + r + 1, :] for r in range(group)],
            axis=1,
        )

    width = group * QUERY_BLOCK
    first = place_ref[0] * tokens + step * QUERY_BLOCK
    query_pos = first + lax.broadcasted_iota(jnp.int32, (1, width), 1) % QUERY_BLOCK

    pool_end = (
        lax.broadcasted_iota(jnp.int32, (pool_count, width), 0) * POOL_BLOCK + POOL_BLOCK - 1
    )
    dq_pool, dk, dv = branch_back(
        pooled_k[...], pooled_v[...], query_stack, gated(0), log_row(0),
        pool_end <= query_pos, scale,
    )
    pool_dk[...] += dk
    pool_dv[...] += dv

    ids = [lists_ref[head, step * CHOSEN + c] for c in range(CHOSEN)]
    rows = [pl.ds(pl.multiple_of(i * KEY_BLOCK, KEY_BLOCK), KEY_BLOCK) for i in ids]
    keys = jnp.concatenate([k_ref[r, :] for r in rows], axis=0)
    values = jnp.concatenate([v_ref[r, :] for r in rows], axis=0)
    offset = lax.broadcasted_iota(jnp.int32, (KEY_BLOCK, width), 0)
    key_pos = jnp.concatenate([offset + i * KEY_BLOCK for i in ids], axis=0)
    dq_pick, dk, dv = branch_back(
        keys, values, query_stack, gated(1), log_row(1), key_pos <= query_pos, scale
    )
    both = jnp.concatenate([dk, dv], axis=1)
    for c in range(CHOSEN):
        part = both[c * KEY_BLOCK : (c + 1) * KEY_BLOCK]
        slot = pl.multiple_of(slot_ref[head, step * CHOSEN + c], KEY_BLOCK)
        own = pl.multiple_of(own_ref[head, step * CHOSEN + c], KEY_BLOCK)
        send_ref[pl.ds(slot, KEY_BLOCK), :] = part.astype(BF16)
        kept[pl.ds(own, KEY_BLOCK), :] += part

    dq = (dq_pool + dq_pick) * scale
    for r in range(group):
        dq_ref[:, r * HEAD_DIM : (r + 1) * HEAD_DIM] = dq[
            :, r * QUERY_BLOCK : (r + 1) * QUERY_BLOCK
        ].T.astype(BF16)

    @pl.when(step == pl.num_programs(1) - 1)
    def _():
        kept_ref[...] = kept[:tokens, :]
        for owner in range(kv_count):
            at = owner * section + CAP * KEY_BLOCK
            here = slice(owner * pool_here, (owner + 1) * pool_here)
            send_ref[at : at + pool_here, :HEAD_DIM] = pool_dk[here, :].astype(BF16)
            send_ref[at : at + pool_here, HEAD_DIM:] = pool_dv[here, :].astype(BF16)


def grid_of(count):
    width = 1
    while width * width * 4 <= count:
        width *= 2
    while count % width:
        width //= 2
    return count // width, width


def meet(peers):
    barrier = pltpu.get_barrier_semaphore()
    for peer in peers:
        pl.semaphore_signal(barrier, inc=1, device_id=peer, device_id_type=MESH)
    pl.semaphore_wait(barrier, len(peers))


def gather_kernel(
    kv_count, tp_count,
    k_ref, v_ref, hidden_ref, list_ref,
    k_all, v_all, hidden_all, list_all,
    z_send, z_recv, y_send, y_recv, h_send, h_recv, l_send, l_recv, own_sem,
):
    nz, ny = grid_of(kv_count)
    me = lax.axis_index("kv")
    tp = lax.axis_index("tp")
    z = me // ny
    y = lax.rem(me, ny)
    tokens = k_ref.shape[0]
    hidden_rows = hidden_ref.shape[0]
    meet(
        [{"kv": lax.rem(me + d, kv_count)} for d in range(1, kv_count)]
        + [{"tp": lax.rem(tp + d, tp_count)} for d in range(1, tp_count)]
    )
    parts = ((k_ref, k_all), (v_ref, v_all))

    def rows_of(row, col):
        return pl.ds(pl.multiple_of((row * ny + col) * tokens, tokens), tokens)

    def source(p, s, row):
        return parts[p][0] if s == 0 else parts[p][1].at[rows_of(row, y)]

    def z_copy(p, side, s, row):
        to = z + 1 if side == 0 else z - 1
        return pltpu.make_async_remote_copy(
            src_ref=source(p, s, row),
            dst_ref=parts[p][1].at[rows_of(row, y)],
            send_sem=z_send.at[p, side, s],
            recv_sem=z_recv.at[p, side, s + 1],
            device_id={"kv": to * ny + y},
            device_id_type=MESH,
        )

    def y_copy(p, side, s, d, row):
        return pltpu.make_async_remote_copy(
            src_ref=source(p, s, row),
            dst_ref=parts[p][1].at[rows_of(row, y)],
            send_sem=y_send.at[p, side, s, d - 1],
            recv_sem=y_recv.at[p, side, s, d - 1],
            device_id={"kv": z * ny + lax.rem(y + d, ny)},
            device_id_type=MESH,
        )

    def h_copy(d):
        at = pl.ds(pl.multiple_of(tp * hidden_rows, hidden_rows), hidden_rows)
        return pltpu.make_async_remote_copy(
            src_ref=hidden_ref,
            dst_ref=hidden_all.at[at],
            send_sem=h_send.at[d - 1],
            recv_sem=h_recv.at[d - 1],
            device_id={"tp": lax.rem(tp + d, tp_count)},
            device_id_type=MESH,
        )

    def l_copy(d):
        return pltpu.make_async_remote_copy(
            src_ref=list_ref,
            dst_ref=list_all.at[me],
            send_sem=l_send.at[d - 1],
            recv_sem=l_recv.at[d - 1],
            device_id={"kv": lax.rem(me + d, kv_count)},
            device_id_type=MESH,
        )

    def spread(side, s):
        row = z - s if side == 0 else z + s
        last = z < nz - 1 if side == 0 else z > 0
        for p in range(2):
            @pl.when(last)
            def _():
                z_copy(p, side, s, row).start()

            if s > 0 or side == 0:
                for d in range(1, ny):
                    y_copy(p, side, s, d, row).start()

    spread(0, 0)
    spread(1, 0)
    for d in range(1, tp_count):
        h_copy(d).start()
    for d in range(1, kv_count):
        l_copy(d).start()
    own = [
        pltpu.make_async_copy(k_ref, k_all.at[rows_of(z, y)], own_sem.at[0]),
        pltpu.make_async_copy(v_ref, v_all.at[rows_of(z, y)], own_sem.at[1]),
        pltpu.make_async_copy(
            hidden_ref,
            hidden_all.at[pl.ds(pl.multiple_of(tp * hidden_rows, hidden_rows), hidden_rows)],
            own_sem.at[2],
        ),
        pltpu.make_async_copy(list_ref, list_all.at[me], own_sem.at[3]),
    ]
    for copy in own:
        copy.start()

    def there(side, s):
        return z >= s if side == 0 else z + s < nz

    for s in range(1, nz):
        for side in range(2):
            @pl.when(there(side, s))
            def _():
                row = z - s if side == 0 else z + s
                for p in range(2):
                    z_copy(p, side, s - 1, row).wait_recv()
                spread(side, s)

    for s in range(nz):
        for side in range(2):
            if s == 0 and side == 1:
                @pl.when(z > 0)
                def _():
                    for p in range(2):
                        z_copy(p, 1, 0, z).wait_send()

                continue

            @pl.when(there(side, s))
            def _():
                row = z - s if side == 0 else z + s
                last = z < nz - 1 if side == 0 else z > 0
                for p in range(2):
                    for d in range(1, ny):
                        y_copy(p, side, s, d, row).wait()

                    @pl.when(last)
                    def _():
                        z_copy(p, side, s, row).wait_send()

    for d in range(1, tp_count):
        h_copy(d).wait()
    for d in range(1, kv_count):
        l_copy(d).wait()
    for copy in own:
        copy.wait()


def weight_kernel(
    kv_count, section,
    hidden_ref, dq_ref, send_ref,
    gw_ref, got_ref,
    tile, turned, acc, y_out, y_in, z_out, z_in,
    tile_sem, ys_sem, yr_sem, zs_sem, zr_sem, as_sem, ar_sem,
):
    nz, ny = grid_of(kv_count)
    me = lax.axis_index("kv")
    z = me // ny
    y = lax.rem(me, ny)
    rows, cols = gw_ref.shape
    width = min(256, cols)
    right = nz - 1 - z
    meet([{"kv": lax.rem(me + d, kv_count)} for d in range(1, kv_count)])

    def owner_row(i):
        return jnp.where(i < right, nz - 1 - i, i - right)

    def exchange(dz, dy):
        to = lax.rem(z + dz, nz) * ny + lax.rem(y + dy, ny)
        n = dz * ny + dy
        return pltpu.make_async_remote_copy(
            src_ref=send_ref.at[pl.ds(pl.multiple_of(to * section, 32), section)],
            dst_ref=got_ref.at[pl.ds(pl.multiple_of(me * section, 32), section)],
            send_sem=as_sem.at[n],
            recv_sem=ar_sem.at[n],
            device_id={"kv": to},
            device_id_type=MESH,
        )

    jobs = [(i, d) for i in range(nz) for d in range(1, ny)] + [(i, 0) for i in range(nz)]

    def fetch(n):
        i, d = jobs[n]
        owner = owner_row(i) * ny + lax.rem(y + d, ny)
        at = pl.ds(pl.multiple_of(owner * rows, rows), rows)
        return pltpu.make_async_copy(hidden_ref.at[:, at], tile.at[n % 2], tile_sem.at[n % 2])

    def ready(n):
        fetch(n).wait()
        turned[...] = tile[n % 2].T
        if n + 1 < len(jobs):
            fetch(n + 1).start()

    def product(c):
        at = pl.ds(pl.multiple_of(c * width, width), width)
        return at, dot_nn(turned[...], dq_ref[:, at])

    def y_copy(i, d):
        return pltpu.make_async_remote_copy(
            src_ref=y_out.at[i, d - 1],
            dst_ref=y_in.at[i, d - 1],
            send_sem=ys_sem.at[i, d - 1],
            recv_sem=yr_sem.at[i, d - 1],
            device_id={"kv": z * ny + lax.rem(y + d, ny)},
            device_id_type=MESH,
        )

    def slot(i):
        return jnp.where(i < right, 0, nz) + owner_row(i)

    def z_copy(i):
        return pltpu.make_async_remote_copy(
            src_ref=z_out.at[i],
            dst_ref=z_in.at[slot(i)],
            send_sem=zs_sem.at[i],
            recv_sem=zr_sem.at[slot(i)],
            device_id={"kv": jnp.where(i < right, z + 1, z - 1) * ny + y},
            device_id_type=MESH,
        )

    def z_came(at):
        return pltpu.make_async_remote_copy(
            src_ref=z_out.at[0],
            dst_ref=z_in.at[at],
            send_sem=zs_sem.at[0],
            recv_sem=zr_sem.at[at],
            device_id={"kv": lax.rem(me + ny, kv_count)},
            device_id_type=MESH,
        )

    fetch(0).start()
    for dz in range(1, nz):
        exchange(dz, 0).start()
    for n, (i, d) in enumerate(jobs):
        if d == 0:
            break
        ready(n)

        def far(c, carry):
            at, part = product(c)
            y_out[i, d - 1, :, at] = part.astype(BF16)
            return carry

        lax.fori_loop(0, cols // width, far, 0)
        y_copy(i, d).start()
    for dy in range(1, ny):
        for dz in range(nz):
            exchange(dz, dy).start()

    for i in range(nz):
        ready(nz * (ny - 1) + i)
        for d in range(1, ny):
            y_copy(i, d).wait_recv()

        def near(c, carry):
            at, part = product(c)
            for d in range(1, ny):
                part = part + y_in[i, d - 1, :, at].astype(F32)
            acc[:, at] = part
            return carry

        lax.fori_loop(0, cols // width, near, 0)
        if i < nz - 1:
            came = jnp.where(i < right, z > 0, z < nz - 1)

            @pl.when(came)
            def _():
                z_came(slot(i)).wait_recv()
                z_out[i] = (acc[...] + z_in[slot(i)].astype(F32)).astype(BF16)

            @pl.when(jnp.logical_not(came))
            def _():
                z_out[i] = acc[...].astype(BF16)

            z_copy(i).start()

    @pl.when(z > 0)
    def _():
        z_came(z).wait_recv()
        acc[...] += z_in[z].astype(F32)

    @pl.when(z < nz - 1)
    def _():
        z_came(nz + z).wait_recv()
        acc[...] += z_in[nz + z].astype(F32)

    gw_ref[...] = acc[...]
    for i in range(nz):
        for d in range(1, ny):
            y_copy(i, d).wait_send()
        if i < nz - 1:
            z_copy(i).wait_send()
    for dz in range(nz):
        for dy in range(ny):
            if dz or dy:
                exchange(dz, dy).wait()


def settle_kernel(
    section, kv_count, place_ref, asked_ref, got_ref, own_ref, kept_ref, gk_ref, gv_ref, acc
):
    head = pl.program_id(0)
    tokens = kept_ref.shape[0]
    pool_here = tokens // POOL_BLOCK
    at = CAP * KEY_BLOCK
    pooled = own_ref[at : at + pool_here, :].astype(F32)
    for i in range(1, kv_count):
        other = lax.rem(place_ref[0] + i, kv_count)
        rows = pl.ds(pl.multiple_of(other * section + at, POOL_BLOCK), pool_here)
        pooled += got_ref[rows, :].astype(F32)
    pooled = pooled / POOL_BLOCK
    for j in range(pool_here):
        rows = slice(j * POOL_BLOCK, (j + 1) * POOL_BLOCK)
        acc[rows, :] = kept_ref[rows, :] + pooled[j : j + 1, :]

    def source(i, carry):
        other = lax.rem(place_ref[0] + 1 + i, kv_count)
        for c in range(CAP):
            block = asked_ref[head, other * CAP + c]
            rows = pl.ds(pl.multiple_of(block * KEY_BLOCK, KEY_BLOCK), KEY_BLOCK)
            came = pl.ds(pl.multiple_of(other * section + c * KEY_BLOCK, KEY_BLOCK), KEY_BLOCK)
            acc[rows, :] += got_ref[came, :].astype(F32)
        return carry

    lax.fori_loop(0, kv_count - 1, source, 0)
    gk_ref[...] = acc[:, :HEAD_DIM].astype(BF16)
    gv_ref[...] = acc[:, HEAD_DIM:].astype(BF16)


def body(hidden_rows, queries, key_rows, value_rows, branch_gates, log_sums, chosen, out_grad):
    kv_count = lax.axis_size("kv")
    kv_index = lax.axis_index("kv")
    tokens = queries.shape[0]
    kv_local = key_rows.shape[1] // HEAD_DIM
    group = HEADS // KV_HEADS
    scale = HEAD_DIM ** (-0.5)
    seq_len = tokens * kv_count
    steps = tokens // QUERY_BLOCK
    blocks_here = tokens // KEY_BLOCK
    pool_count = seq_len // POOL_BLOCK
    pool_here = tokens // POOL_BLOCK
    request_count = steps * CHOSEN
    section = CAP * KEY_BLOCK + pool_here
    slot_count = kv_count * CAP

    lists = chosen.reshape(kv_local, request_count)
    tp_count = lax.axis_size("tp")
    nz, ny = grid_of(kv_count)
    dma = pltpu.SemaphoreType.DMA
    anywhere = pl.BlockSpec(memory_space=pl.ANY)
    inside = pl.BlockSpec(memory_space=pltpu.VMEM)
    k_all, v_all, hidden_all, list_all = pl.pallas_call(
        functools.partial(gather_kernel, kv_count, tp_count),
        in_specs=[inside] * 4,
        out_specs=[anywhere, anywhere, anywhere, inside],
        out_shape=[
            jax.ShapeDtypeStruct((seq_len, key_rows.shape[1]), BF16),
            jax.ShapeDtypeStruct((seq_len, key_rows.shape[1]), BF16),
            jax.ShapeDtypeStruct((tokens, hidden_rows.shape[1]), BF16),
            jax.ShapeDtypeStruct((kv_count, kv_local, request_count), jnp.int32),
        ],
        scratch_shapes=[
            dma((2, 2, nz)), dma((2, 2, nz + 1)),
            dma((2, 2, nz, max(ny - 1, 1))), dma((2, 2, nz, max(ny - 1, 1))),
            dma((tp_count - 1,)), dma((tp_count - 1,)),
            dma((kv_count - 1,)), dma((kv_count - 1,)),
            dma((4,)),
        ],
        compiler_params=pltpu.CompilerParams(
            collective_id=0, has_side_effects=True, vmem_limit_bytes=VMEM_LIMIT
        ),
        name="gather",
    )(key_rows, value_rows, hidden_rows, lists)
    owners = lists // blocks_here
    local_block = lists % blocks_here
    remote = owners != kv_index
    order = jnp.arange(request_count, dtype=jnp.int32)
    rank_in = jnp.sum(
        (
            (owners[:, :, None] == owners[:, None, :]) & (order[None, None, :] < order[None, :, None])
        ).astype(jnp.int32),
        axis=-1,
    )
    named = list_all.transpose(1, 0, 2)
    mine = (named // blocks_here == kv_index).astype(jnp.int32)
    ahead = jnp.sum(
        mine[:, :, None, :] * (order[None, None, None, :] < order[None, None, :, None]), axis=-1
    )
    asked_for = jnp.sum(
        jnp.where(
            (mine[:, :, None, :] > 0)
            & (ahead[:, :, None, :] == jnp.arange(CAP, dtype=jnp.int32)[None, None, :, None]),
            named[:, :, None, :] % blocks_here,
            0,
        ),
        axis=-1,
    ).reshape(kv_local, slot_count)
    slot_row = jnp.where(remote, owners * section + rank_in * KEY_BLOCK, kv_index * section)
    own_row = jnp.where(remote, tokens, local_block * KEY_BLOCK)
    place = kv_index.astype(jnp.int32).reshape(1)

    def per_head(array):
        return (
            array.reshape(2, kv_local, group, tokens)
            .transpose(1, 0, 2, 3)
            .reshape(kv_local, 2 * group, tokens)
        )

    pairs_flops = 2 * kv_local * group * tokens * HEAD_DIM * (pool_count + CHOSEN * KEY_BLOCK) * 5
    wide = 2 * HEAD_DIM
    grad_queries, send, kept = pl.pallas_call(
        functools.partial(attend_kernel, group, section, kv_count, scale),
        grid_spec=pltpu.PrefetchScalarGridSpec(
            num_scalar_prefetch=4,
            grid=(kv_local, steps),
            in_specs=[
                pl.BlockSpec((QUERY_BLOCK, group * HEAD_DIM), lambda h, b, *_: (b, h)),
                pl.BlockSpec((QUERY_BLOCK, group * HEAD_DIM), lambda h, b, *_: (b, h)),
                pl.BlockSpec((1, 2 * group, QUERY_BLOCK), lambda h, b, *_: (h, 0, b)),
                pl.BlockSpec((1, 2 * group, QUERY_BLOCK), lambda h, b, *_: (h, 0, b)),
                pl.BlockSpec((seq_len, HEAD_DIM), lambda h, b, *_: (0, h)),
                pl.BlockSpec((seq_len, HEAD_DIM), lambda h, b, *_: (0, h)),
            ],
            out_specs=[
                pl.BlockSpec((QUERY_BLOCK, group * HEAD_DIM), lambda h, b, *_: (b, h)),
                pl.BlockSpec((kv_count * section, wide), lambda h, b, *_: (0, h)),
                pl.BlockSpec((tokens, wide), lambda h, b, *_: (0, h)),
            ],
            scratch_shapes=[
                pltpu.VMEM((pool_count, HEAD_DIM), BF16),
                pltpu.VMEM((pool_count, HEAD_DIM), BF16),
                pltpu.VMEM((pool_count, HEAD_DIM), F32),
                pltpu.VMEM((pool_count, HEAD_DIM), F32),
                pltpu.VMEM((tokens + KEY_BLOCK, wide), F32),
            ],
        ),
        out_shape=[
            jax.ShapeDtypeStruct((tokens, kv_local * group * HEAD_DIM), BF16),
            jax.ShapeDtypeStruct((kv_count * section, kv_local * wide), BF16),
            jax.ShapeDtypeStruct((tokens, kv_local * wide), F32),
        ],
        cost_estimate=pl.CostEstimate(
            flops=pairs_flops, bytes_accessed=24 * 2**20, transcendentals=0
        ),
        name="attend_back",
    )(
        place, lists, slot_row, own_row,
        queries, out_grad, per_head(branch_gates), per_head(log_sums), k_all, v_all,
    )

    model = hidden_rows.shape[1]
    out_rows = model // kv_count
    out_cols = grad_queries.shape[1]
    unit = (out_rows, out_cols)
    far = max(ny - 1, 1)
    grad_weight, got = pl.pallas_call(
        functools.partial(weight_kernel, kv_count, section),
        in_specs=[anywhere, inside, anywhere],
        out_specs=[inside, anywhere],
        out_shape=[
            jax.ShapeDtypeStruct(unit, F32),
            jax.ShapeDtypeStruct(send.shape, BF16),
        ],
        scratch_shapes=[
            pltpu.VMEM((2, tokens, out_rows), BF16),
            pltpu.VMEM((out_rows, tokens), BF16),
            pltpu.VMEM(unit, F32),
            pltpu.VMEM((nz, far) + unit, BF16),
            pltpu.VMEM((nz, far) + unit, BF16),
            pltpu.VMEM((nz,) + unit, BF16),
            pltpu.VMEM((2 * nz,) + unit, BF16),
            dma((2,)), dma((nz, far)), dma((nz, far)), dma((nz,)), dma((2 * nz,)),
            dma((kv_count,)), dma((kv_count,)),
        ],
        compiler_params=pltpu.CompilerParams(
            collective_id=1, has_side_effects=True, vmem_limit_bytes=VMEM_LIMIT
        ),
        name="weight",
    )(hidden_all, grad_queries, send)

    grad_keys, grad_values = pl.pallas_call(
        functools.partial(settle_kernel, section, kv_count),
        grid_spec=pltpu.PrefetchScalarGridSpec(
            num_scalar_prefetch=2,
            grid=(kv_local,),
            in_specs=[
                pl.BlockSpec((kv_count * section, wide), lambda h, *_: (0, h)),
                pl.BlockSpec((section, wide), lambda h, place, *_: (place[0], h)),
                pl.BlockSpec((tokens, wide), lambda h, *_: (0, h)),
            ],
            out_specs=[
                pl.BlockSpec((tokens, HEAD_DIM), lambda h, *_: (0, h)),
                pl.BlockSpec((tokens, HEAD_DIM), lambda h, *_: (0, h)),
            ],
            scratch_shapes=[pltpu.VMEM((tokens, wide), F32)],
        ),
        out_shape=[
            jax.ShapeDtypeStruct((tokens, kv_local * HEAD_DIM), BF16),
            jax.ShapeDtypeStruct((tokens, kv_local * HEAD_DIM), BF16),
        ],
        cost_estimate=pl.CostEstimate(
            flops=4 * 2**20, bytes_accessed=8 * 2**20, transcendentals=0
        ),
        name="settle",
    )(place, asked_for, got, send, kept)
    return (grad_queries, grad_keys, grad_values, grad_weight)


def solution(mesh):
    placed = (
        P(("kv", "tp"), None),
        P("kv", "tp"),
        P("kv", "tp"),
        P("kv", "tp"),
        P(None, "tp", "kv"),
        P(None, "tp", "kv"),
        P("tp", "kv", None),
        P("kv", "tp"),
    )
    return jax.shard_map(
        body,
        mesh=mesh,
        in_specs=placed,
        out_specs=(P("kv", "tp"), P("kv", "tp"), P("kv", "tp"), P("kv", "tp")),
        check_vma=False,
    )
```

```python
import functools

import jax
import jax.numpy as jnp
from jax import lax
from jax.experimental import pallas as pl
from jax.experimental.pallas import tpu as pltpu
from jax.sharding import PartitionSpec as P

HEADS = 32
KV_HEADS = 8
HEAD_DIM = 128
QUERY_BLOCK = 128
KEY_BLOCK = 32
POOL_BLOCK = 32
CHOSEN = 16
CAP = 16

F32 = jnp.float32
BF16 = jnp.bfloat16
MESH = pl.DeviceIdType.MESH
VMEM_LIMIT = 62 * 2**20


def dot_nt(a, b):
    return lax.dot_general(a, b, (((1,), (1,)), ((), ())), preferred_element_type=F32)


def dot_nn(a, b):
    return lax.dot_general(a, b, (((1,), (0,)), ((), ())), preferred_element_type=F32)


def branch_back(keys, values, query_stack, cot_stack, log_row, mask, scale):
    scores = dot_nt(keys, query_stack) * scale
    weights = jnp.where(mask, jnp.exp(scores - log_row), 0.0)
    weights_low = weights.astype(BF16)
    grad_prob = dot_nt(values, cot_stack)
    delta = jnp.sum(weights_low.astype(F32) * grad_prob, axis=0, keepdims=True)
    dscore = (weights * (grad_prob - delta)).astype(BF16)
    dquery = dot_nn(keys.T, dscore)
    return dquery, dot_nn(dscore, query_stack) * scale, dot_nn(weights_low, cot_stack)


def grid_of(count):
    width = 1
    while width * width * 4 <= count:
        width *= 2
    while count % width:
        width //= 2
    return count // width, width


def meet(peers):
    barrier = pltpu.get_barrier_semaphore()
    for peer in peers:
        pl.semaphore_signal(barrier, inc=1, device_id=peer, device_id_type=MESH)
    pl.semaphore_wait(barrier, len(peers))


def step_kernel(
    kv_count, tp_count, group, scale,
    lists_ref, slots_ref, own_ref,
    wanted_ref, k_ref, v_ref, hidden_ref, gate_ref, log_ref, q_hbm, g_hbm,
    dq_ref, gw_ref, kept_ref, got_ref, pool_got, asked_ref, hid_all,
    q_buf, g_buf, k_heads, v_heads, pooled, pool_acc, pool_out, dq_pool, dq_far,
    parts, out_box, turned, tile, partial, z_out, z_in,
    in_sem, z_send, z_recv, y_send, y_recv, p_send, p_recv, w_send, w_recv, pg_send, pg_recv,
    hy_send, hy_recv, hx_send, hx_recv, hs_send, hs_recv, dq_send, dq_recv,
    a_send, a_recv, s_send, s_recv,
):
    nz, ny = grid_of(kv_count)
    me = lax.axis_index("kv")
    tp = lax.axis_index("tp")
    z = me // ny
    y = lax.rem(me, ny)
    cores = 2 if tp_count % 2 == 0 else 1
    nx = tp_count // cores
    x = tp // cores
    core = lax.rem(tp, cores)
    blocks_here = k_ref.shape[0]
    tokens = blocks_here * KEY_BLOCK
    heads = k_ref.shape[2] // HEAD_DIM
    steps = tokens // QUERY_BLOCK
    requests = steps * CHOSEN
    pool_count = pooled.shape[0] * pooled.shape[1]
    pool_here = pooled.shape[1]
    hidden_rows = hidden_ref.shape[0]
    rows, cols = gw_ref.shape
    head_cols = group * HEAD_DIM
    wide = 2 * HEAD_DIM
    width = group * QUERY_BLOCK
    box = CAP * KEY_BLOCK
    meet(
        [{"kv": lax.rem(me + d, kv_count)} for d in range(1, kv_count)]
        + [{"tp": lax.rem(tp + d, tp_count)} for d in range(1, tp_count)]
    )
    banks = ((k_ref, k_heads), (v_ref, v_heads))

    def remote(src, dst, send, recv, to):
        return pltpu.make_async_remote_copy(
            src_ref=src, dst_ref=dst, send_sem=send, recv_sem=recv,
            device_id=to, device_id_type=MESH,
        )

    def rows_of(row, col):
        return pl.ds((row * ny + col) * blocks_here, blocks_here)

    def source(h, p, s, row):
        if s == 0:
            return banks[p][0].at[:, :, h * HEAD_DIM : (h + 1) * HEAD_DIM]
        return banks[p][1][h].at[rows_of(row, y)]

    def z_copy(h, p, side, s, row):
        to = z + 1 if side == 0 else z - 1
        return remote(
            source(h, p, s, row), banks[p][1][h].at[rows_of(row, y)],
            z_send.at[h, p, side, s], z_recv.at[h, p, side, s + 1], {"kv": to * ny + y},
        )

    def y_copy(h, p, side, s, d, row, col):
        return remote(
            source(h, p, s, row), banks[p][1][h].at[rows_of(row, col)],
            y_send.at[h, p, side, s, d - 1], y_recv.at[h, p, side, s, d - 1],
            {"kv": z * ny + lax.rem(y + d, ny)},
        )

    def there(side, s):
        return z >= s if side == 0 else z + s < nz

    def onward(side):
        return z < nz - 1 if side == 0 else z > 0

    def place(side, s):
        return z - s if side == 0 else z + s

    def pass_z(h, side, s):
        @pl.when(onward(side))
        def _():
            for p in range(2):
                z_copy(h, p, side, s, place(side, s)).start()

    def pass_y(h, side, s):
        for p in range(2):
            for d in range(1, ny):
                y_copy(h, p, side, s, d, place(side, s), y).start()

    def relay_keys(h, s):
        if h >= heads:
            return
        for side in range(2):
            @pl.when(there(side, s))
            def _():
                for p in range(2):
                    z_copy(h, p, side, s - 1, place(side, s)).wait_recv()
                pass_z(h, side, s)
                pass_y(h, side, s)

    def keys_complete(h):
        for s in range(nz):
            for side in range(1 if s == 0 else 2):
                @pl.when(there(side, s))
                def _():
                    for p in range(2):
                        for d in range(1, ny):
                            y_copy(h, p, side, s, d, place(side, s), y).wait_recv()

    def others(make):
        return [make(d) for d in range(1, kv_count)]

    def spread(src, dst, send, recv):
        def make(d):
            to = lax.rem(me + d, kv_count)
            return remote(src(to), dst.at[me], send.at[d - 1], recv.at[d - 1], {"kv": to})

        return others(make)

    fetches = [
        pltpu.make_async_copy(q_hbm, q_buf, in_sem.at[0]),
        pltpu.make_async_copy(g_hbm, g_buf, in_sem.at[1]),
        pltpu.make_async_copy(wanted_ref.at[me], asked_ref.at[me], in_sem.at[2]),
    ]
    for h in range(heads):
        for p in range(2):
            fetches.append(
                pltpu.make_async_copy(
                    source(h, p, 0, z), banks[p][1][h].at[rows_of(z, y)],
                    in_sem.at[3 + 2 * h + p],
                )
            )
    hid_local = [
        pltpu.make_async_copy(
            hidden_ref.at[:, pl.ds(pl.multiple_of((row * ny + y) * rows, rows), rows)],
            hid_all.at[row, pl.ds(pl.multiple_of((y * tp_count + tp) * hidden_rows, hidden_rows), hidden_rows)],
            in_sem.at[3 + 2 * heads + row],
        )
        for row in range(nz)
    ]

    def hid_rows(col, part):
        at = (col * tp_count + part) * hidden_rows
        return hid_all.at[:, pl.ds(pl.multiple_of(at, hidden_rows), hidden_rows)]

    def hy_copy(d, row):
        to = lax.rem(y + d, ny)
        return remote(
            hidden_ref.at[:, pl.ds(pl.multiple_of((row * ny + to) * rows, rows), rows)],
            hid_all.at[row, pl.ds(pl.multiple_of((y * tp_count + tp) * hidden_rows, hidden_rows), hidden_rows)],
            hy_send.at[d - 1, row], hy_recv.at[d - 1, row], {"kv": z * ny + to},
        )

    def hx_copy(e, d):
        col = lax.rem(y + ny - e, ny)
        to = lax.rem(x + d, nx) * cores + core
        return remote(
            hid_rows(col, tp), hid_rows(col, tp),
            hx_send.at[e, d - 1], hx_recv.at[e, d - 1], {"tp": to},
        )

    def hs_copy(e, d):
        col = lax.rem(y + ny - e, ny)
        part = lax.rem(x + nx - d, nx) * cores + core
        return remote(
            hid_rows(col, part), hid_rows(col, part),
            hs_send.at[e, d], hs_recv.at[e, d], {"tp": x * cores + 1 - core},
        )

    def hidden_out(e):
        for d in range(1, nx):
            hx_copy(e, d).start()
        if cores > 1:
            hs_copy(e, 0).start()

    def hidden_on(e):
        for d in range(1, nx):
            hx_copy(e, d).wait_recv()
            if cores > 1:
                hs_copy(e, d).start()

    def exchange(h, dz, dy):
        to = lax.rem(z + dz, nz) * ny + lax.rem(y + dy, ny)
        n = dz * ny + dy
        return remote(
            out_box.at[to],
            got_ref.at[h, pl.ds(pl.multiple_of(me * box, box), box)],
            a_send.at[h, n], a_recv.at[h, n], {"kv": to},
        )

    def dq_copy(h, d):
        return remote(
            dq_ref.at[:, h * head_cols : (h + 1) * head_cols], dq_far.at[h, d - 1],
            dq_send.at[h, d - 1], dq_recv.at[h, d - 1],
            {"kv": z * ny + lax.rem(y + d, ny)},
        )

    right = nz - 1 - z
    right_first = z * 2 < nz

    def owner_row(i):
        ahead = jnp.where(i < right, nz - 1 - i, i - right)
        back = jnp.where(i < z, i, nz - 1 - (i - z))
        return jnp.where(right_first, ahead, back)

    def goes_right(i):
        return jnp.where(right_first, jnp.where(i < right, 1, 0), jnp.where(i < z, 0, 1)) > 0

    def sum_copy(h, i):
        to = jnp.where(goes_right(i), z + 1, z - 1)
        slot = jnp.where(goes_right(i), owner_row(i) - to, nz - to + owner_row(i))
        return remote(
            z_out.at[h, i], z_in.at[h, slot], s_send.at[h, i], s_recv.at[h, slot],
            {"kv": to * ny + y},
        )

    def sum_came(h, slot):
        return remote(
            z_out.at[h, 0], z_in.at[h, slot], s_send.at[h, 0], s_recv.at[h, slot],
            {"kv": lax.rem(me + ny, kv_count)},
        )

    def in_slot(i):
        return jnp.where(goes_right(i), owner_row(i) - z, nz - z + owner_row(i))

    def has_in(i):
        return jnp.where(goes_right(i), jnp.where(z > 0, 1, 0), jnp.where(z < nz - 1, 1, 0)) > 0

    pick = (
        lax.broadcasted_iota(jnp.int32, (pool_here, tokens), 1) // POOL_BLOCK
        == lax.broadcasted_iota(jnp.int32, (pool_here, tokens), 0)
    ).astype(BF16)
    for p in range(2):
        mean = (dot_nn(pick, banks[p][0][...].reshape(tokens, heads * HEAD_DIM)) / POOL_BLOCK).astype(BF16)
        pooled[me, :, p * heads * HEAD_DIM : (p + 1) * heads * HEAD_DIM] = mean
    pool_sends = spread(lambda to: pooled.at[me], pooled, p_send, p_recv)
    for copy in pool_sends:
        copy.start()
    want_sends = spread(lambda to: wanted_ref.at[to], asked_ref, w_send, w_recv)
    pass_z(0, 0, 0)
    pass_z(0, 1, 0)
    pass_y(0, 0, 0)
    for copy in fetches + hid_local + want_sends:
        copy.start()
    parts[requests] = jnp.zeros((KEY_BLOCK, wide), BF16)
    pool_acc[...] = jnp.zeros_like(pool_acc)
    for copy in hid_local:
        copy.wait()
    hidden_out(0)
    for copy in fetches:
        copy.wait()
    for copy in pool_sends:
        copy.wait_recv()

    def load_step(h, b, branch):
        at = pl.ds(pl.multiple_of(b * QUERY_BLOCK, QUERY_BLOCK), QUERY_BLOCK)
        first = h * head_cols
        stack = jnp.concatenate(
            [q_buf[at, first + r * HEAD_DIM : first + (r + 1) * HEAD_DIM] for r in range(group)],
            axis=0,
        )
        gates = gate_ref[branch, :, at].T
        cots = jnp.concatenate(
            [
                (
                    gates[:, h * group + r : h * group + r + 1]
                    * g_buf[at, first + r * HEAD_DIM : first + (r + 1) * HEAD_DIM].astype(F32)
                ).astype(BF16)
                for r in range(group)
            ],
            axis=0,
        )
        logs = log_ref[branch, :, at]
        log_row = jnp.concatenate(
            [logs[h * group + r : h * group + r + 1, :] for r in range(group)], axis=1
        )
        query_pos = (
            me * tokens + b * QUERY_BLOCK
            + lax.broadcasted_iota(jnp.int32, (1, width), 1) % QUERY_BLOCK
        )
        return at, stack, cots, log_row, query_pos

    def pool_steps(h, low, high):
        def one(b, carry):
            at, stack, cots, log_row, query_pos = load_step(h, b, 0)
            pool_end = (
                lax.broadcasted_iota(jnp.int32, (pool_count, width), 0) * POOL_BLOCK
                + POOL_BLOCK - 1
            )
            first = h * HEAD_DIM
            keys = pooled[:, :, first : first + HEAD_DIM].reshape(pool_count, HEAD_DIM)
            first += heads * HEAD_DIM
            values = pooled[:, :, first : first + HEAD_DIM].reshape(pool_count, HEAD_DIM)
            dq, dk, dv = branch_back(
                keys, values, stack, cots, log_row, pool_end <= query_pos, scale
            )
            dq_pool[h * steps + b] = dq
            pool_acc[h] += jnp.concatenate([dk, dv], axis=1)
            return carry

        lax.fori_loop(low, high, one, 0)

    def pick_steps(h, low, high):
        def one(b, carry):
            at, stack, cots, log_row, query_pos = load_step(h, b, 1)
            ids = [lists_ref[h, b * CHOSEN + c] for c in range(CHOSEN)]
            keys = jnp.concatenate([k_heads[h][i] for i in ids], axis=0)
            values = jnp.concatenate([v_heads[h][i] for i in ids], axis=0)
            offset = lax.broadcasted_iota(jnp.int32, (KEY_BLOCK, width), 0)
            key_pos = jnp.concatenate([offset + i * KEY_BLOCK for i in ids], axis=0)
            dq, dk, dv = branch_back(
                keys, values, stack, cots, log_row, key_pos <= query_pos, scale
            )
            parts[pl.ds(b * CHOSEN, CHOSEN)] = (
                jnp.concatenate([dk, dv], axis=1).astype(BF16).reshape(CHOSEN, KEY_BLOCK, wide)
            )
            dq = (dq + dq_pool[h * steps + b]) * scale
            for r in range(group):
                first = h * head_cols + r * HEAD_DIM
                dq_ref[at, first : first + HEAD_DIM] = dq[
                    :, r * QUERY_BLOCK : (r + 1) * QUERY_BLOCK
                ].T.astype(BF16)
            return carry

        lax.fori_loop(low, high, one, 0)

    def pack(h):
        def to_owner(d, carry):
            owner = lax.rem(me + d, kv_count)
            for c in range(CAP):
                out_box[owner, c * KEY_BLOCK : (c + 1) * KEY_BLOCK, :] = parts[
                    slots_ref[h, owner * CAP + c]
                ]
            return carry

        lax.fori_loop(1, kv_count, to_owner, 0)

    def keep(h):
        def to_self(b, carry):
            total = parts[own_ref[h, b * steps]].astype(F32)
            for step in range(1, steps):
                total += parts[own_ref[h, b * steps + step]].astype(F32)
            at = pl.ds(pl.multiple_of(b * KEY_BLOCK, KEY_BLOCK), KEY_BLOCK)
            kept_ref[at, h * wide : (h + 1) * wide] = total
            return carry

        lax.fori_loop(0, blocks_here, to_self, 0)

    def send_boxes(h, near):
        for dy in range(1) if near else range(1, ny):
            for dz in range(1 if dy == 0 else 0, nz):
                exchange(h, dz, dy).start()

    def weigh(h, i):
        lane = min(256, head_cols)

        def one(c, carry):
            at = pl.ds(pl.multiple_of(c * lane, lane), lane)
            mine = pl.ds(pl.multiple_of(y * tokens, tokens), tokens)
            from_self = pl.ds(pl.multiple_of(h * head_cols + c * lane, lane), lane)
            total = dot_nn(turned[i, :, mine], dq_ref[:, from_self])
            for d in range(1, ny):
                theirs = pl.ds(pl.multiple_of(lax.rem(y + ny - d, ny) * tokens, tokens), tokens)
                total += dot_nn(turned[i, :, theirs], dq_far[h, d - 1, :, at])
            if i < nz - 1:
                partial[i, :, at] = total
            else:
                gw_ref[:, from_self] = total
            return carry

        lax.fori_loop(0, head_cols // lane, one, 0)

    def sum_first(h):
        for d in range(1, ny):
            dq_copy(h, d).wait_recv()
        for i in range(nz):
            weigh(h, i)
            if i < nz - 1:
                @pl.when(jnp.logical_not(has_in(i)))
                def _():
                    z_out[h, i] = partial[i].astype(BF16)
                    sum_copy(h, i).start()

    def sum_relay(h, i):
        @pl.when(has_in(i))
        def _():
            sum_came(h, in_slot(i)).wait_recv()
            z_out[h, i] = (partial[i] + z_in[h, in_slot(i)].astype(F32)).astype(BF16)
            sum_copy(h, i).start()

    def sum_last(h):
        at = slice(h * head_cols, (h + 1) * head_cols)
        for slot, some in ((0, z > 0), (nz, z < nz - 1)):
            @pl.when(some)
            def _():
                sum_came(h, slot).wait_recv()
                gw_ref[:, at] += z_in[h, slot].astype(F32)

    half = max(steps * 3 // 4, 1)
    pool_steps(0, 0, half)
    relay_keys(0, 1)
    pool_steps(0, half, steps)
    for h in range(1, heads):
        pool_steps(h, 0, steps)
    relay_keys(0, 2)
    if heads > 1:
        pass_z(1, 0, 0)
        pass_z(1, 1, 0)
    for h in range(heads):
        pool_out[:, :, h * wide : (h + 1) * wide] = (
            pool_acc[h].astype(BF16).reshape(kv_count, pool_here, wide)
        )
    for s in range(3, nz):
        relay_keys(0, s)
    for row in range(nz):
        for d in range(1, ny):
            hy_copy(d, row).start()
    if heads > 1:
        pass_y(1, 0, 0)
    pool_grads = spread(lambda to: pool_out.at[to], pool_got, pg_send, pg_recv)
    for copy in pool_grads:
        copy.start()
    own_pool = pltpu.make_async_copy(pool_out.at[me], pool_got.at[me], in_sem.at[0])
    own_pool.start()
    hidden_on(0)

    for h in range(heads):
        if h + 1 < heads:
            relay_keys(h + 1, 1)
        keys_complete(h)
        cuts = [steps * (i + 1) // nz for i in range(nz)]
        low = 0
        for i, cut in enumerate(cuts):
            pick_steps(h, low, cut)
            low = cut
            if h > 0 and i < nz - 1:
                sum_relay(h - 1, i)
            if i == nz // 2 and nz > 2:
                relay_keys(h + 1, 2)
        for d in range(1, ny):
            dq_copy(h, d).start()
        if h > 0:
            for dz in range(nz):
                for dy in range(ny):
                    if dz or dy:
                        exchange(h - 1, dz, dy).wait_send()
        pack(h)
        send_boxes(h, True)
        if h + 1 < heads:
            for s in range(3, nz):
                relay_keys(h + 1, s)
            if h + 2 < heads:
                pass_z(h + 2, 0, 0)
                pass_z(h + 2, 1, 0)
                pass_y(h + 2, 0, 0)
        send_boxes(h, False)
        keep(h)
        if h == 0:
            for d in range(1, ny):
                for row in range(nz):
                    hy_copy(d, row).wait_recv()
                hidden_out(d)
            for d in range(1, ny):
                hidden_on(d)
            if cores > 1:
                for e in range(ny):
                    for d in range(nx):
                        hs_copy(e, d).wait_recv()
            for i in range(nz):
                grab = pltpu.make_async_copy(hid_all.at[owner_row(i)], tile, in_sem.at[1])
                grab.start()
                grab.wait()
                turned[i] = tile[...].T
        sum_first(h)
    for i in range(nz - 1):
        sum_relay(heads - 1, i)
    for h in range(heads):
        sum_last(h)

    own_pool.wait()
    for copy in pool_sends:
        copy.wait_send()
    for copy in want_sends + pool_grads:
        copy.wait()
    for h in range(heads):
        for s in range(nz):
            for side in range(2):
                @pl.when(there(side, s))
                def _():
                    @pl.when(onward(side))
                    def _():
                        for p in range(2):
                            z_copy(h, p, side, s, place(side, s)).wait_send()

                    if s > 0 or side == 0:
                        for p in range(2):
                            for d in range(1, ny):
                                y_copy(h, p, side, s, d, place(side, s), y).wait_send()

        for d in range(1, ny):
            dq_copy(h, d).wait_send()
        for dz in range(nz):
            for dy in range(ny):
                if dz or dy:
                    if h == heads - 1:
                        exchange(h, dz, dy).wait_send()
                    exchange(h, dz, dy).wait_recv()
        for i in range(nz - 1):
            sum_copy(h, i).wait_send()
    for d in range(1, ny):
        for row in range(nz):
            hy_copy(d, row).wait_send()
    for e in range(ny):
        for d in range(1, nx):
            hx_copy(e, d).wait_send()
        if cores > 1:
            for d in range(nx):
                hs_copy(e, d).wait_send()


def settle_kernel(
    kv_count, place_ref, asked_ref, got_ref, pool_ref, kept_ref, gk_ref, gv_ref, acc
):
    head = pl.program_id(0)
    tokens = kept_ref.shape[0]
    pool_here = tokens // POOL_BLOCK
    box = CAP * KEY_BLOCK
    pooled = sum(pool_ref[i].astype(F32) for i in range(kv_count)) / POOL_BLOCK
    for j in range(pool_here):
        rows = slice(j * POOL_BLOCK, (j + 1) * POOL_BLOCK)
        acc[rows, :] = kept_ref[rows, :] + pooled[j : j + 1, :]

    def source(i, carry):
        other = lax.rem(place_ref[0] + 1 + i, kv_count)
        for c in range(CAP):
            block = asked_ref[other, head * CAP + c]
            rows = pl.ds(pl.multiple_of(block * KEY_BLOCK, KEY_BLOCK), KEY_BLOCK)
            came = pl.ds(pl.multiple_of(other * box + c * KEY_BLOCK, KEY_BLOCK), KEY_BLOCK)
            acc[rows, :] += got_ref[0, came, :].astype(F32)
        return carry

    lax.fori_loop(0, kv_count - 1, source, 0)
    gk_ref[...] = acc[:, :HEAD_DIM].astype(BF16)
    gv_ref[...] = acc[:, HEAD_DIM:].astype(BF16)


def body(hidden_rows, queries, key_rows, value_rows, branch_gates, log_sums, chosen, out_grad):
    kv_count = lax.axis_size("kv")
    tp_count = lax.axis_size("tp")
    kv_index = lax.axis_index("kv")
    tokens = queries.shape[0]
    kv_local = key_rows.shape[1] // HEAD_DIM
    group = HEADS // KV_HEADS
    scale = HEAD_DIM ** (-0.5)
    seq_len = tokens * kv_count
    steps = tokens // QUERY_BLOCK
    blocks_here = tokens // KEY_BLOCK
    pool_here = tokens // POOL_BLOCK
    request_count = steps * CHOSEN
    slot_count = kv_count * CAP
    nz, ny = grid_of(kv_count)

    lists = chosen.reshape(kv_local, request_count)
    owners = lists // blocks_here
    local_block = lists % blocks_here
    remote = owners != kv_index
    order = jnp.arange(request_count, dtype=jnp.int32)
    rank_in = jnp.sum(
        (
            (owners[:, :, None] == owners[:, None, :]) & (order[None, None, :] < order[None, :, None])
        ).astype(jnp.int32),
        axis=-1,
    )
    slot_index = jnp.where(remote, owners * CAP + rank_in, slot_count)
    hit = slot_index[:, None, :] == jnp.arange(slot_count, dtype=jnp.int32)[None, :, None]
    slot_from = request_count + jnp.sum(jnp.where(hit, order - request_count, 0), axis=-1)
    wanted = jnp.sum(jnp.where(hit, local_block[:, None, :], 0), axis=-1)
    wanted = (
        wanted.reshape(kv_local, kv_count, CAP).transpose(1, 0, 2).reshape(kv_count, 1, -1)
    )
    wanted = jnp.pad(wanted, ((0, 0), (0, 0), (0, 128 - kv_local * CAP)))
    own_block = jnp.where(remote, -1, local_block).reshape(kv_local, 1, steps, CHOSEN)
    same = own_block == jnp.arange(blocks_here, dtype=jnp.int32)[None, :, None, None]
    own_from = (
        request_count
        + jnp.sum(jnp.where(same, order.reshape(steps, CHOSEN) - request_count, 0), axis=-1)
    ).reshape(kv_local, blocks_here * steps)
    place = kv_index.astype(jnp.int32).reshape(1)

    wide = 2 * HEAD_DIM
    box = CAP * KEY_BLOCK
    model = hidden_rows.shape[1]
    out_rows = model // kv_count
    head_cols = group * HEAD_DIM
    out_cols = kv_local * head_cols
    far = max(ny - 1, 1)
    cores = 2 if tp_count % 2 == 0 else 1
    nx = tp_count // cores
    side = max(nx - 1, 1)
    dma = pltpu.SemaphoreType.DMA
    anywhere = pl.BlockSpec(memory_space=pl.ANY)
    inside = pl.BlockSpec(memory_space=pltpu.VMEM)
    scalars = pl.BlockSpec(memory_space=pltpu.SMEM)
    vmem = pltpu.VMEM
    out = jax.ShapeDtypeStruct
    grad_queries, grad_weight, kept, got, pool_got, asked, _ = pl.pallas_call(
        functools.partial(step_kernel, kv_count, tp_count, group, scale),
        in_specs=[scalars] * 3 + [inside] * 6 + [anywhere] * 2,
        out_specs=[inside, inside, inside, anywhere, anywhere, inside, anywhere],
        out_shape=[
            out((tokens, out_cols), BF16),
            out((out_rows, out_cols), F32),
            out((tokens, kv_local * wide), F32),
            out((kv_local, kv_count * box, wide), BF16),
            out((kv_count, pool_here, kv_local * wide), BF16),
            out((kv_count, 1, 128), jnp.int32),
            out((nz, ny * tokens, out_rows), BF16),
        ],
        scratch_shapes=[
            vmem((tokens, out_cols), BF16),
            vmem((tokens, out_cols), BF16),
            [vmem((seq_len // KEY_BLOCK, KEY_BLOCK, HEAD_DIM), BF16) for _ in range(kv_local)],
            [vmem((seq_len // KEY_BLOCK, KEY_BLOCK, HEAD_DIM), BF16) for _ in range(kv_local)],
            vmem((kv_count, pool_here, kv_local * wide), BF16),
            vmem((kv_local, kv_count * pool_here, wide), F32),
            vmem((kv_count, pool_here, kv_local * wide), BF16),
            vmem((kv_local * steps, HEAD_DIM, group * QUERY_BLOCK), F32),
            vmem((kv_local, far, tokens, head_cols), BF16),
            vmem((request_count + 1, KEY_BLOCK, wide), BF16),
            vmem((kv_count, box, wide), BF16),
            vmem((nz, out_rows, ny * tokens), BF16),
            vmem((ny * tokens, out_rows), BF16),
            vmem((max(nz - 1, 1), out_rows, head_cols), F32),
            vmem((kv_local, max(nz - 1, 1), out_rows, head_cols), BF16),
            vmem((kv_local, nz + 1, out_rows, head_cols), BF16),
            dma((3 + 2 * kv_local + nz,)),
            dma((kv_local, 2, 2, nz)), dma((kv_local, 2, 2, nz + 1)),
            dma((kv_local, 2, 2, nz, far)), dma((kv_local, 2, 2, nz, far)),
            dma((kv_count,)), dma((kv_count,)), dma((kv_count,)), dma((kv_count,)),
            dma((kv_count,)), dma((kv_count,)),
            dma((far, nz)), dma((far, nz)), dma((ny, side)), dma((ny, side)),
            dma((ny, nx)), dma((ny, nx)), dma((kv_local, far)), dma((kv_local, far)),
            dma((kv_local, kv_count)), dma((kv_local, kv_count)),
            dma((kv_local, nz)), dma((kv_local, nz + 1)),
        ],
        compiler_params=pltpu.CompilerParams(
            collective_id=0, has_side_effects=True, vmem_limit_bytes=VMEM_LIMIT
        ),
        name="step",
    )(
        lists, slot_from, own_from,
        wanted,
        key_rows.reshape(blocks_here, KEY_BLOCK, kv_local * HEAD_DIM),
        value_rows.reshape(blocks_here, KEY_BLOCK, kv_local * HEAD_DIM),
        hidden_rows, branch_gates, log_sums, queries, out_grad,
    )

    grad_keys, grad_values = pl.pallas_call(
        functools.partial(settle_kernel, kv_count),
        grid_spec=pltpu.PrefetchScalarGridSpec(
            num_scalar_prefetch=2,
            grid=(kv_local,),
            in_specs=[
                pl.BlockSpec((1, kv_count * box, wide), lambda h, *_: (h, 0, 0)),
                pl.BlockSpec((kv_count, pool_here, wide), lambda h, *_: (0, 0, h)),
                pl.BlockSpec((tokens, wide), lambda h, *_: (0, h)),
            ],
            out_specs=[
                pl.BlockSpec((tokens, HEAD_DIM), lambda h, *_: (0, h)),
                pl.BlockSpec((tokens, HEAD_DIM), lambda h, *_: (0, h)),
            ],
            scratch_shapes=[pltpu.VMEM((tokens, wide), F32)],
        ),
        out_shape=[
            jax.ShapeDtypeStruct((tokens, kv_local * HEAD_DIM), BF16),
            jax.ShapeDtypeStruct((tokens, kv_local * HEAD_DIM), BF16),
        ],
        cost_estimate=pl.CostEstimate(
            flops=4 * 2**20, bytes_accessed=8 * 2**20, transcendentals=0
        ),
        name="settle",
    )(place, asked.reshape(kv_count, 128), got, pool_got, kept)
    return (grad_queries, grad_keys, grad_values, grad_weight)


def solution(mesh):
    placed = (
        P(("kv", "tp"), None),
        P("kv", "tp"),
        P("kv", "tp"),
        P("kv", "tp"),
        P(None, "tp", "kv"),
        P(None, "tp", "kv"),
        P("tp", "kv", None),
        P("kv", "tp"),
    )
    return jax.shard_map(
        body,
        mesh=mesh,
        in_specs=placed,
        out_specs=(P("kv", "tp"), P("kv", "tp"), P("kv", "tp"), P("kv", "tp")),
        check_vma=False,
    )
```

```python
import functools

import jax
import jax.numpy as jnp
from jax import lax
from jax.experimental import pallas as pl
from jax.experimental.pallas import tpu as pltpu
from jax.sharding import PartitionSpec as P

HEADS = 32
KV_HEADS = 8
HEAD_DIM = 128
QUERY_BLOCK = 128
KEY_BLOCK = 32
POOL_BLOCK = 32
CHOSEN = 16
CAP = 16

F32 = jnp.float32
BF16 = jnp.bfloat16
MESH = pl.DeviceIdType.MESH
VMEM_LIMIT = 67043328


def dot_nt(a, b):
    return lax.dot_general(a, b, (((1,), (1,)), ((), ())), preferred_element_type=F32)


def dot_nn(a, b):
    return lax.dot_general(a, b, (((1,), (0,)), ((), ())), preferred_element_type=F32)


def branch_back(keys, values, query_stack, cot_stack, log_row, mask, scale):
    scores = dot_nt(keys, query_stack) * scale
    weights = jnp.where(mask, jnp.exp(scores - log_row), 0.0)
    weights_low = weights.astype(BF16)
    grad_prob = dot_nt(values, cot_stack)
    delta = jnp.sum(weights_low.astype(F32) * grad_prob, axis=0, keepdims=True)
    dscore = (weights * (grad_prob - delta)).astype(BF16)
    dquery = dot_nn(keys.T, dscore)
    return dquery, dot_nn(dscore, query_stack) * scale, dot_nn(weights_low, cot_stack)


def grid_of(count):
    width = 1
    while width * width * 4 <= count:
        width *= 2
    while count % width:
        width //= 2
    return count // width, width


def meet(peers):
    barrier = pltpu.get_barrier_semaphore()
    for peer in peers:
        pl.semaphore_signal(barrier, inc=1, device_id=peer, device_id_type=MESH)
    pl.semaphore_wait(barrier, len(peers))


def step_kernel(
    kv_count, tp_count, group, scale,
    lists_ref, spots_ref, slots_ref, own_ref,
    wanted_ref, k_ref, v_ref, gate_ref, log_ref, hidden_ref, q_hbm, g_hbm,
    dq_ref, gw_ref, kept_ref, got_ref, pool_got, asked_ref, hid_all,
    q_buf, g_buf, kv_all, kv_own, kv_in, kv_out, want_in, want,
    pooled, pool_acc, pool_out, dq_pool, dq_far,
    parts, out_box, turned, tile, partial, z_out, z_in,
    in_sem, z_send, z_recv, y_send, y_recv, t_send, t_recv,
    p_send, p_recv, w_send, w_recv, pg_send, pg_recv,
    hy_send, hy_recv, hx_send, hx_recv, hs_send, hs_recv, dq_send, dq_recv,
    a_send, a_recv, s_send, s_recv,
):
    nz, ny = grid_of(kv_count)
    me = lax.axis_index("kv")
    tp = lax.axis_index("tp")
    z = me // ny
    y = lax.rem(me, ny)
    cores = 2 if tp_count % 2 == 0 else 1
    nx = tp_count // cores
    x = tp // cores
    core = lax.rem(tp, cores)
    blocks_here = k_ref.shape[0]
    tokens = blocks_here * KEY_BLOCK
    heads = k_ref.shape[2] // HEAD_DIM
    steps = tokens // QUERY_BLOCK
    requests = steps * CHOSEN
    pool_count = pooled.shape[0] * pooled.shape[1]
    pool_here = pooled.shape[1]
    hidden_rows = hidden_ref.shape[0]
    rows, cols = gw_ref.shape
    head_cols = group * HEAD_DIM
    wide = 2 * HEAD_DIM
    width = group * QUERY_BLOCK
    box = CAP * KEY_BLOCK
    own_keys = (k_ref, v_ref)
    for h in range(heads):
        for p in range(2):
            kv_own[h, p] = own_keys[p][:, :, h * HEAD_DIM : (h + 1) * HEAD_DIM]
    meet(
        [{"kv": lax.rem(me + d, kv_count)} for d in range(1, kv_count)]
        + [{"tp": lax.rem(tp + d, tp_count)} for d in range(1, tp_count)]
    )

    def remote(src, dst, send, recv, to):
        return pltpu.make_async_remote_copy(
            src_ref=src, dst_ref=dst, send_sem=send, recv_sem=recv,
            device_id=to, device_id_type=MESH,
        )

    def source(h, side, s):
        return kv_own.at[h] if s == 0 else kv_in[h][side][s - 1]

    def z_copy(h, side, s):
        to = z + 1 if side == 0 else z - 1
        return remote(
            source(h, side, s), kv_in[h][side][s],
            z_send.at[h, side, s], z_recv.at[h, side, s], {"kv": to * ny + y},
        )

    def y_copy(h, row, d):
        at = nz * blocks_here + (row * (ny - 1) + d - 1) * CAP
        return remote(
            kv_out.at[h, row, d - 1], kv_all[h].at[:, pl.ds(at, CAP)],
            y_send.at[h, row, d - 1], y_recv.at[h, row, d - 1],
            {"kv": z * ny + lax.rem(y + d, ny)},
        )

    def t_copy(d):
        return remote(
            wanted_ref, want_in.at[d - 1], t_send.at[d - 1], t_recv.at[d - 1],
            {"kv": z * ny + lax.rem(y + d, ny)},
        )

    def there(side, s):
        return z >= s if side == 0 else z + s < nz

    def onward(side):
        return z < nz - 1 if side == 0 else z > 0

    def pass_z(h, side, s):
        if s < nz - 1:
            @pl.when(onward(side))
            def _():
                z_copy(h, side, s).start()

    def pass_y(h, side, s):
        row = z - s if side == 0 else z + s
        held = source(h, side, s)
        kv_all[h][:, pl.ds(row * blocks_here, blocks_here)] = held[...]
        for d in range(1, ny):
            for c in range(CAP):
                block = want[ny - d - 1, row * ny + y, 0, h * CAP + c]
                for p in range(2):
                    kv_out[h, row, d - 1, p, c] = held[p, block]
            y_copy(h, row, d).start()

    def relay_keys(h, s):
        if h >= heads:
            return
        for side in range(2):
            @pl.when(there(side, s))
            def _():
                z_copy(h, side, s - 1).wait_recv()
                pass_z(h, side, s)

        for side in range(2):
            @pl.when(there(side, s))
            def _():
                pass_y(h, side, s)

    def keys_complete(h):
        for row in range(nz):
            for d in range(1, ny):
                y_copy(h, row, d).wait_recv()

    def others(make):
        return [make(d) for d in range(1, kv_count)]

    def spread(src, dst, send, recv):
        def make(d):
            to = lax.rem(me + d, kv_count)
            return remote(src(to), dst.at[me], send.at[d - 1], recv.at[d - 1], {"kv": to})

        return others(make)

    fetches = [
        pltpu.make_async_copy(q_hbm, q_buf, in_sem.at[0]),
        pltpu.make_async_copy(g_hbm, g_buf, in_sem.at[1]),
        pltpu.make_async_copy(wanted_ref.at[me], asked_ref.at[me], in_sem.at[2]),
    ]
    def hid_piece(row):
        return tile.at[row * hidden_rows : (row + 1) * hidden_rows]

    hid_local = [
        pltpu.make_async_copy(
            hidden_ref.at[:, pl.ds(pl.multiple_of((row * ny + y) * rows, rows), rows)],
            hid_piece(row),
            in_sem.at[3 + row],
        )
        for row in range(nz)
    ]
    hid_home = [
        pltpu.make_async_copy(
            hid_piece(row),
            hid_all.at[row, pl.ds(pl.multiple_of((y * tp_count + tp) * hidden_rows, hidden_rows), hidden_rows)],
            in_sem.at[3 + row],
        )
        for row in range(nz)
    ]

    def hid_rows(col, part):
        at = (col * tp_count + part) * hidden_rows
        return hid_all.at[:, pl.ds(pl.multiple_of(at, hidden_rows), hidden_rows)]

    def hy_copy(d, row):
        to = lax.rem(y + d, ny)
        return remote(
            hidden_ref.at[:, pl.ds(pl.multiple_of((row * ny + to) * rows, rows), rows)],
            hid_all.at[row, pl.ds(pl.multiple_of((y * tp_count + tp) * hidden_rows, hidden_rows), hidden_rows)],
            hy_send.at[d - 1, row], hy_recv.at[d - 1, row], {"kv": z * ny + to},
        )

    def hx_copy(e, d):
        col = lax.rem(y + ny - e, ny)
        to = lax.rem(x + d, nx) * cores + core
        return remote(
            hid_rows(col, tp), hid_rows(col, tp),
            hx_send.at[e, d - 1], hx_recv.at[e, d - 1], {"tp": to},
        )

    def hs_copy(e, d):
        col = lax.rem(y + ny - e, ny)
        part = lax.rem(x + nx - d, nx) * cores + core
        return remote(
            hid_rows(col, part), hid_rows(col, part),
            hs_send.at[e, d], hs_recv.at[e, d], {"tp": x * cores + 1 - core},
        )

    def hidden_out(e):
        for d in range(1, nx):
            hx_copy(e, d).start()
        if cores > 1:
            hs_copy(e, 0).start()

    def hidden_on(e):
        for d in range(1, nx):
            hx_copy(e, d).wait_recv()
            if cores > 1:
                hs_copy(e, d).start()

    def exchange(h, dz, dy):
        to = lax.rem(z + dz, nz) * ny + lax.rem(y + dy, ny)
        n = dz * ny + dy
        return remote(
            out_box.at[to],
            got_ref.at[h, pl.ds(pl.multiple_of(me * box, box), box)],
            a_send.at[h, n], a_recv.at[h, n], {"kv": to},
        )

    def dq_copy(h, d):
        return remote(
            dq_ref.at[:, h * head_cols : (h + 1) * head_cols], dq_far.at[h, d - 1],
            dq_send.at[h, d - 1], dq_recv.at[h, d - 1],
            {"kv": z * ny + lax.rem(y + d, ny)},
        )

    right = nz - 1 - z
    right_first = z * 2 < nz

    def owner_row(i):
        ahead = jnp.where(i < right, nz - 1 - i, i - right)
        back = jnp.where(i < z, i, nz - 1 - (i - z))
        return jnp.where(right_first, ahead, back)

    def goes_right(i):
        return jnp.where(right_first, jnp.where(i < right, 1, 0), jnp.where(i < z, 0, 1)) > 0

    def sum_copy(h, i):
        to = jnp.where(goes_right(i), z + 1, z - 1)
        slot = jnp.where(goes_right(i), owner_row(i) - to, nz - to + owner_row(i))
        return remote(
            z_out.at[h, i], z_in.at[h, slot], s_send.at[h, i], s_recv.at[h, slot],
            {"kv": to * ny + y},
        )

    def sum_came(h, slot):
        return remote(
            z_out.at[h, 0], z_in.at[h, slot], s_send.at[h, 0], s_recv.at[h, slot],
            {"kv": lax.rem(me + ny, kv_count)},
        )

    def in_slot(i):
        return jnp.where(goes_right(i), owner_row(i) - z, nz - z + owner_row(i))

    def has_in(i):
        return jnp.where(goes_right(i), jnp.where(z > 0, 1, 0), jnp.where(z < nz - 1, 1, 0)) > 0

    pass_z(0, 0, 0)
    pass_z(0, 1, 0)
    for d in range(1, ny):
        t_copy(d).start()
    pick = (
        lax.broadcasted_iota(jnp.int32, (pool_here, tokens), 1) // POOL_BLOCK
        == lax.broadcasted_iota(jnp.int32, (pool_here, tokens), 0)
    ).astype(BF16)
    for p in range(2):
        all_rows = own_keys[p][...].reshape(tokens, heads * HEAD_DIM)
        mean = (dot_nn(pick, all_rows) / POOL_BLOCK).astype(BF16)
        pooled[me, :, p * heads * HEAD_DIM : (p + 1) * heads * HEAD_DIM] = mean
    pool_sends = spread(lambda to: pooled.at[me], pooled, p_send, p_recv)
    for copy in pool_sends:
        copy.start()
    want_sends = spread(lambda to: wanted_ref.at[to], asked_ref, w_send, w_recv)
    for copy in fetches + hid_local + want_sends:
        copy.start()
    parts[requests] = jnp.zeros((KEY_BLOCK, wide), BF16)
    pool_acc[...] = jnp.zeros_like(pool_acc)
    for there_copy, home_copy in zip(hid_local, hid_home):
        there_copy.wait()
        home_copy.start()
    for copy in hid_home:
        copy.wait()
    hidden_out(0)
    for d in range(1, ny):
        t_copy(d).wait_recv()
    for copy in fetches:
        copy.wait()
    to_scalar = pltpu.make_async_copy(want_in, want, in_sem.at[0])
    to_scalar.start()
    to_scalar.wait()
    pass_y(0, 0, 0)

    def hy_start(row):
        if row < nz:
            for d in range(1, ny):
                hy_copy(d, row).start()

    hy_start(0)
    for copy in pool_sends:
        copy.wait_recv()

    def load_step(h, b, branch):
        at = pl.ds(pl.multiple_of(b * QUERY_BLOCK, QUERY_BLOCK), QUERY_BLOCK)
        first = h * head_cols
        stack = jnp.concatenate(
            [q_buf[at, first + r * HEAD_DIM : first + (r + 1) * HEAD_DIM] for r in range(group)],
            axis=0,
        )
        gates = gate_ref[branch, :, at].T
        cots = jnp.concatenate(
            [
                (
                    gates[:, h * group + r : h * group + r + 1]
                    * g_buf[at, first + r * HEAD_DIM : first + (r + 1) * HEAD_DIM].astype(F32)
                ).astype(BF16)
                for r in range(group)
            ],
            axis=0,
        )
        logs = log_ref[branch, :, at]
        log_row = jnp.concatenate(
            [logs[h * group + r : h * group + r + 1, :] for r in range(group)], axis=1
        )
        query_pos = (
            me * tokens + b * QUERY_BLOCK
            + lax.broadcasted_iota(jnp.int32, (1, width), 1) % QUERY_BLOCK
        )
        return at, stack, cots, log_row, query_pos

    def pool_steps(h, low, high):
        def one(b, carry):
            at, stack, cots, log_row, query_pos = load_step(h, b, 0)
            pool_end = (
                lax.broadcasted_iota(jnp.int32, (pool_count, width), 0) * POOL_BLOCK
                + POOL_BLOCK - 1
            )
            first = h * HEAD_DIM
            keys = pooled[:, :, first : first + HEAD_DIM].reshape(pool_count, HEAD_DIM)
            first += heads * HEAD_DIM
            values = pooled[:, :, first : first + HEAD_DIM].reshape(pool_count, HEAD_DIM)
            dq, dk, dv = branch_back(
                keys, values, stack, cots, log_row, pool_end <= query_pos, scale
            )
            dq_pool[h * steps + b] = dq
            pool_acc[h] += jnp.concatenate([dk, dv], axis=1)
            return carry

        lax.fori_loop(low, high, one, 0)

    def pick_steps(h, low, high):
        def one(b, carry):
            at, stack, cots, log_row, query_pos = load_step(h, b, 1)
            ids = [lists_ref[h, b * CHOSEN + c] for c in range(CHOSEN)]
            spots = [spots_ref[h, b * CHOSEN + c] for c in range(CHOSEN)]
            keys = jnp.concatenate([kv_all[h][0, i] for i in spots], axis=0)
            values = jnp.concatenate([kv_all[h][1, i] for i in spots], axis=0)
            offset = lax.broadcasted_iota(jnp.int32, (KEY_BLOCK, width), 0)
            key_pos = jnp.concatenate([offset + i * KEY_BLOCK for i in ids], axis=0)
            dq, dk, dv = branch_back(
                keys, values, stack, cots, log_row, key_pos <= query_pos, scale
            )
            parts[pl.ds(b * CHOSEN, CHOSEN)] = (
                jnp.concatenate([dk, dv], axis=1).astype(BF16).reshape(CHOSEN, KEY_BLOCK, wide)
            )
            dq = (dq + dq_pool[h * steps + b]) * scale
            for r in range(group):
                first = h * head_cols + r * HEAD_DIM
                dq_ref[at, first : first + HEAD_DIM] = dq[
                    :, r * QUERY_BLOCK : (r + 1) * QUERY_BLOCK
                ].T.astype(BF16)
            return carry

        lax.fori_loop(low, high, one, 0)

    def pack(h):
        def to_owner(d, carry):
            owner = lax.rem(me + d, kv_count)
            for c in range(CAP):
                out_box[owner, c * KEY_BLOCK : (c + 1) * KEY_BLOCK, :] = parts[
                    slots_ref[h, owner * CAP + c]
                ]
            return carry

        lax.fori_loop(1, kv_count, to_owner, 0)

    def keep(h):
        def to_self(b, carry):
            total = parts[own_ref[h, b * steps]].astype(F32)
            for step in range(1, steps):
                total += parts[own_ref[h, b * steps + step]].astype(F32)
            at = pl.ds(pl.multiple_of(b * KEY_BLOCK, KEY_BLOCK), KEY_BLOCK)
            kept_ref[at, h * wide : (h + 1) * wide] = total
            return carry

        lax.fori_loop(0, blocks_here, to_self, 0)

    def send_boxes(h, near):
        for dy in range(1) if near else range(1, ny):
            for dz in range(1 if dy == 0 else 0, nz):
                exchange(h, dz, dy).start()

    def weigh(h, i):
        lane = min(256, head_cols)

        def one(c, carry):
            at = pl.ds(pl.multiple_of(c * lane, lane), lane)
            mine = pl.ds(pl.multiple_of(y * tokens, tokens), tokens)
            from_self = pl.ds(pl.multiple_of(h * head_cols + c * lane, lane), lane)
            total = dot_nn(turned[i, :, mine], dq_ref[:, from_self])
            for d in range(1, ny):
                theirs = pl.ds(pl.multiple_of(lax.rem(y + ny - d, ny) * tokens, tokens), tokens)
                total += dot_nn(turned[i, :, theirs], dq_far[h, d - 1, :, at])
            if i < nz - 1:
                partial[i, :, at] = total
            else:
                gw_ref[:, from_self] = total
            return carry

        lax.fori_loop(0, head_cols // lane, one, 0)

    def sum_first(h):
        for d in range(1, ny):
            dq_copy(h, d).wait_recv()
        for i in range(nz):
            weigh(h, i)
            if i < nz - 1:
                @pl.when(jnp.logical_not(has_in(i)))
                def _():
                    z_out[h, i] = partial[i].astype(BF16)
                    sum_copy(h, i).start()

    def sum_relay(h, i):
        @pl.when(has_in(i))
        def _():
            sum_came(h, in_slot(i)).wait_recv()
            z_out[h, i] = (partial[i] + z_in[h, in_slot(i)].astype(F32)).astype(BF16)
            sum_copy(h, i).start()

    def sum_last(h):
        at = slice(h * head_cols, (h + 1) * head_cols)
        for slot, some in ((0, z > 0), (nz, z < nz - 1)):
            @pl.when(some)
            def _():
                sum_came(h, slot).wait_recv()
                gw_ref[:, at] += z_in[h, slot].astype(F32)

    half = max(steps * 3 // 4, 1)
    pool_steps(0, 0, half)
    relay_keys(0, 1)
    hy_start(1)
    pool_steps(0, half, steps)
    for h in range(1, heads):
        pool_steps(h, 0, steps)
    for s in range(2, nz):
        relay_keys(0, s)
        hy_start(s)
        if s == 2 and heads > 1:
            pass_z(1, 0, 0)
            pass_z(1, 1, 0)
            pass_y(1, 0, 0)
    for h in range(heads):
        pool_out[:, :, h * wide : (h + 1) * wide] = (
            pool_acc[h].astype(BF16).reshape(kv_count, pool_here, wide)
        )
    pool_grads = spread(lambda to: pool_out.at[to], pool_got, pg_send, pg_recv)
    for copy in pool_grads:
        copy.start()
    own_pool = pltpu.make_async_copy(pool_out.at[me], pool_got.at[me], in_sem.at[0])
    own_pool.start()
    hidden_on(0)

    def hidden_arrived():
        for d in range(1, ny):
            for row in range(nz):
                hy_copy(d, row).wait_recv()
            hidden_out(d)

    def hidden_ready():
        for d in range(1, ny):
            hidden_on(d)
        if cores > 1:
            for e in range(ny):
                for d in range(nx):
                    hs_copy(e, d).wait_recv()
        for i in range(nz):
            for col in range(ny):
                at = pl.ds(col * tokens, tokens)
                grab = pltpu.make_async_copy(hid_all.at[owner_row(i), at], tile, in_sem.at[1])
                grab.start()
                grab.wait()
                turned[i, :, col * tokens : (col + 1) * tokens] = tile[...].T

    for h in range(heads):
        keys_complete(h)
        cuts = [max(steps // 4, 1), max(steps // 2, 1), steps * 7 // 8, steps]
        low = 0
        for i, high in enumerate(cuts):
            pick_steps(h, low, high)
            low = high
            if h > 0:
                sums = [j for j in range(nz - 1) if min(j, 2) == i]
                for j in sums:
                    sum_relay(h - 1, j)
            if i == 0:
                relay_keys(h + 1, 1)
                if h == 0:
                    hidden_arrived()
            if i == 2:
                relay_keys(h + 1, 2)
        for d in range(1, ny):
            dq_copy(h, d).start()
        if h > 0:
            for dz in range(nz):
                for dy in range(ny):
                    if dz or dy:
                        exchange(h - 1, dz, dy).wait_send()
        pack(h)
        send_boxes(h, True)
        for s in range(3, nz):
            relay_keys(h + 1, s)
        if h + 2 < heads:
            pass_z(h + 2, 0, 0)
            pass_z(h + 2, 1, 0)
            pass_y(h + 2, 0, 0)
        keep(h)
        if h == 0:
            hidden_ready()
        sum_first(h)
        send_boxes(h, False)
    for i in range(nz - 1):
        sum_relay(heads - 1, i)
    for h in range(heads):
        sum_last(h)

    own_pool.wait()
    for copy in pool_sends:
        copy.wait_send()
    for copy in want_sends + pool_grads:
        copy.wait()
    for d in range(1, ny):
        t_copy(d).wait_send()
    for h in range(heads):
        for s in range(nz - 1):
            for side in range(2):
                @pl.when(there(side, s))
                def _():
                    @pl.when(onward(side))
                    def _():
                        z_copy(h, side, s).wait_send()

        for row in range(nz):
            for d in range(1, ny):
                y_copy(h, row, d).wait_send()
        for d in range(1, ny):
            dq_copy(h, d).wait_send()
        for dz in range(nz):
            for dy in range(ny):
                if dz or dy:
                    if h == heads - 1:
                        exchange(h, dz, dy).wait_send()
                    exchange(h, dz, dy).wait_recv()
        for i in range(nz - 1):
            sum_copy(h, i).wait_send()
    for d in range(1, ny):
        for row in range(nz):
            hy_copy(d, row).wait_send()
    for e in range(ny):
        for d in range(1, nx):
            hx_copy(e, d).wait_send()
        if cores > 1:
            for d in range(nx):
                hs_copy(e, d).wait_send()


def settle_kernel(
    kv_count, place_ref, asked_ref, got_ref, pool_ref, kept_ref, gk_ref, gv_ref, acc
):
    head = pl.program_id(0)
    tokens = kept_ref.shape[0]
    pool_here = tokens // POOL_BLOCK
    box = CAP * KEY_BLOCK
    pooled = sum(pool_ref[i].astype(F32) for i in range(kv_count)) / POOL_BLOCK
    for j in range(pool_here):
        rows = slice(j * POOL_BLOCK, (j + 1) * POOL_BLOCK)
        acc[rows, :] = kept_ref[rows, :] + pooled[j : j + 1, :]

    def source(i, carry):
        other = lax.rem(place_ref[0] + 1 + i, kv_count)
        for c in range(CAP):
            block = asked_ref[other, head * CAP + c]
            rows = pl.ds(pl.multiple_of(block * KEY_BLOCK, KEY_BLOCK), KEY_BLOCK)
            came = pl.ds(pl.multiple_of(other * box + c * KEY_BLOCK, KEY_BLOCK), KEY_BLOCK)
            acc[rows, :] += got_ref[0, came, :].astype(F32)
        return carry

    lax.fori_loop(0, kv_count - 1, source, 0)
    gk_ref[...] = acc[:, :HEAD_DIM].astype(BF16)
    gv_ref[...] = acc[:, HEAD_DIM:].astype(BF16)


def body(hidden_rows, queries, key_rows, value_rows, branch_gates, log_sums, chosen, out_grad):
    kv_count = lax.axis_size("kv")
    tp_count = lax.axis_size("tp")
    kv_index = lax.axis_index("kv")
    tokens = queries.shape[0]
    kv_local = key_rows.shape[1] // HEAD_DIM
    group = HEADS // KV_HEADS
    scale = HEAD_DIM ** (-0.5)
    seq_len = tokens * kv_count
    steps = tokens // QUERY_BLOCK
    blocks_here = tokens // KEY_BLOCK
    pool_here = tokens // POOL_BLOCK
    request_count = steps * CHOSEN
    slot_count = kv_count * CAP
    nz, ny = grid_of(kv_count)

    lists = chosen.reshape(kv_local, request_count)
    owners = lists // blocks_here
    local_block = lists % blocks_here
    remote = owners != kv_index
    order = jnp.arange(request_count, dtype=jnp.int32)
    rank_in = jnp.sum(
        (
            (owners[:, :, None] == owners[:, None, :]) & (order[None, None, :] < order[None, :, None])
        ).astype(jnp.int32),
        axis=-1,
    )
    slot_index = jnp.where(remote, owners * CAP + rank_in, slot_count)
    hit = slot_index[:, None, :] == jnp.arange(slot_count, dtype=jnp.int32)[None, :, None]
    slot_from = request_count + jnp.sum(jnp.where(hit, order - request_count, 0), axis=-1)
    wanted = jnp.sum(jnp.where(hit, local_block[:, None, :], 0), axis=-1)
    wanted = (
        wanted.reshape(kv_local, kv_count, CAP).transpose(1, 0, 2).reshape(kv_count, 1, -1)
    )
    wanted = jnp.pad(wanted, ((0, 0), (0, 0), (0, 128 - kv_local * CAP)))
    own_block = jnp.where(remote, -1, local_block).reshape(kv_local, 1, steps, CHOSEN)
    same = own_block == jnp.arange(blocks_here, dtype=jnp.int32)[None, :, None, None]
    own_from = (
        request_count
        + jnp.sum(jnp.where(same, order.reshape(steps, CHOSEN) - request_count, 0), axis=-1)
    ).reshape(kv_local, blocks_here * steps)
    place = kv_index.astype(jnp.int32).reshape(1)
    row, col = owners // ny, owners % ny
    here = kv_index % ny
    away = (here - col + ny) % ny
    spots = jnp.where(
        away == 0,
        row * blocks_here + local_block,
        nz * blocks_here + (row * (ny - 1) + away - 1) * CAP + rank_in,
    )

    wide = 2 * HEAD_DIM
    box = CAP * KEY_BLOCK
    model = hidden_rows.shape[1]
    out_rows = model // kv_count
    head_cols = group * HEAD_DIM
    out_cols = kv_local * head_cols
    far = max(ny - 1, 1)
    cores = 2 if tp_count % 2 == 0 else 1
    nx = tp_count // cores
    side = max(nx - 1, 1)
    dma = pltpu.SemaphoreType.DMA
    anywhere = pl.BlockSpec(memory_space=pl.ANY)
    inside = pl.BlockSpec(memory_space=pltpu.VMEM)
    scalars = pl.BlockSpec(memory_space=pltpu.SMEM)
    vmem = pltpu.VMEM
    out = jax.ShapeDtypeStruct
    grad_queries, grad_weight, kept, got, pool_got, asked, _ = pl.pallas_call(
        functools.partial(step_kernel, kv_count, tp_count, group, scale),
        in_specs=[scalars] * 4 + [inside] * 5 + [anywhere] * 3,
        out_specs=[inside, inside, inside, anywhere, anywhere, inside, anywhere],
        out_shape=[
            out((tokens, out_cols), BF16),
            out((out_rows, out_cols), F32),
            out((tokens, kv_local * wide), F32),
            out((kv_local, kv_count * box, wide), BF16),
            out((kv_count, pool_here, kv_local * wide), BF16),
            out((kv_count, 1, 128), jnp.int32),
            out((nz, ny * tokens, out_rows), BF16),
        ],
        scratch_shapes=[
            vmem((tokens, out_cols), BF16),
            vmem((tokens, out_cols), BF16),
            [
                vmem((2, nz * (blocks_here + (ny - 1) * CAP), KEY_BLOCK, HEAD_DIM), BF16)
                for _ in range(kv_local)
            ],
            vmem((kv_local, 2, blocks_here, KEY_BLOCK, HEAD_DIM), BF16),
            [
                [
                    [vmem((2, blocks_here, KEY_BLOCK, HEAD_DIM), BF16) for _ in range(nz - 1)]
                    for _ in range(2)
                ]
                for _ in range(kv_local)
            ],
            vmem((kv_local, nz, far, 2, CAP, KEY_BLOCK, HEAD_DIM), BF16),
            vmem((far, kv_count, 1, 128), jnp.int32),
            pltpu.SMEM((far, kv_count, 1, 128), jnp.int32),
            vmem((kv_count, pool_here, kv_local * wide), BF16),
            vmem((kv_local, kv_count * pool_here, wide), F32),
            vmem((kv_count, pool_here, kv_local * wide), BF16),
            vmem((kv_local * steps, HEAD_DIM, group * QUERY_BLOCK), F32),
            vmem((kv_local, far, tokens, head_cols), BF16),
            vmem((request_count + 1, KEY_BLOCK, wide), BF16),
            vmem((kv_count, box, wide), BF16),
            vmem((nz, out_rows, ny * tokens), BF16),
            vmem((tokens, out_rows), BF16),
            vmem((max(nz - 1, 1), out_rows, head_cols), F32),
            vmem((kv_local, max(nz - 1, 1), out_rows, head_cols), BF16),
            vmem((kv_local, nz + 1, out_rows, head_cols), BF16),
            dma((3 + nz,)),
            dma((kv_local, 2, nz)), dma((kv_local, 2, nz)),
            dma((kv_local, nz, far)), dma((kv_local, nz, far)), dma((far,)), dma((far,)),
            dma((kv_count,)), dma((kv_count,)), dma((kv_count,)), dma((kv_count,)),
            dma((kv_count,)), dma((kv_count,)),
            dma((far, nz)), dma((far, nz)), dma((ny, side)), dma((ny, side)),
            dma((ny, nx)), dma((ny, nx)), dma((kv_local, far)), dma((kv_local, far)),
            dma((kv_local, kv_count)), dma((kv_local, kv_count)),
            dma((kv_local, nz)), dma((kv_local, nz + 1)),
        ],
        compiler_params=pltpu.CompilerParams(
            collective_id=0, has_side_effects=True, vmem_limit_bytes=VMEM_LIMIT
        ),
        name="step",
    )(
        lists, spots, slot_from, own_from,
        wanted,
        key_rows.reshape(blocks_here, KEY_BLOCK, kv_local * HEAD_DIM),
        value_rows.reshape(blocks_here, KEY_BLOCK, kv_local * HEAD_DIM),
        branch_gates, log_sums, hidden_rows, queries, out_grad,
    )

    grad_keys, grad_values = pl.pallas_call(
        functools.partial(settle_kernel, kv_count),
        grid_spec=pltpu.PrefetchScalarGridSpec(
            num_scalar_prefetch=2,
            grid=(kv_local,),
            in_specs=[
                pl.BlockSpec((1, kv_count * box, wide), lambda h, *_: (h, 0, 0)),
                pl.BlockSpec((kv_count, pool_here, wide), lambda h, *_: (0, 0, h)),
                pl.BlockSpec((tokens, wide), lambda h, *_: (0, h)),
            ],
            out_specs=[
                pl.BlockSpec((tokens, HEAD_DIM), lambda h, *_: (0, h)),
                pl.BlockSpec((tokens, HEAD_DIM), lambda h, *_: (0, h)),
            ],
            scratch_shapes=[pltpu.VMEM((tokens, wide), F32)],
        ),
        out_shape=[
            jax.ShapeDtypeStruct((tokens, kv_local * HEAD_DIM), BF16),
            jax.ShapeDtypeStruct((tokens, kv_local * HEAD_DIM), BF16),
        ],
        cost_estimate=pl.CostEstimate(
            flops=4 * 2**20, bytes_accessed=8 * 2**20, transcendentals=0
        ),
        name="settle",
    )(place, asked.reshape(kv_count, 128), got, pool_got, kept)
    return (grad_queries, grad_keys, grad_values, grad_weight)


def solution(mesh):
    placed = (
        P(("kv", "tp"), None),
        P("kv", "tp"),
        P("kv", "tp"),
        P("kv", "tp"),
        P(None, "tp", "kv"),
        P(None, "tp", "kv"),
        P("tp", "kv", None),
        P("kv", "tp"),
    )
    return jax.shard_map(
        body,
        mesh=mesh,
        in_specs=placed,
        out_specs=(P("kv", "tp"), P("kv", "tp"), P("kv", "tp"), P("kv", "tp")),
        check_vma=False,
    )
```

```python
import functools

import jax
import jax.numpy as jnp
from jax import lax
from jax.experimental import pallas as pl
from jax.experimental.pallas import tpu as pltpu
from jax.sharding import PartitionSpec as P

HEADS = 32
KV_HEADS = 8
HEAD_DIM = 128
QUERY_BLOCK = 128
KEY_BLOCK = 32
POOL_BLOCK = 32
CHOSEN = 16
CAP = 16

F32 = jnp.float32
BF16 = jnp.bfloat16
MESH = pl.DeviceIdType.MESH
VMEM_LIMIT = 67043328


def dot_nt(a, b):
    return lax.dot_general(a, b, (((1,), (1,)), ((), ())), preferred_element_type=F32)


def dot_nn(a, b):
    return lax.dot_general(a, b, (((1,), (0,)), ((), ())), preferred_element_type=F32)


def branch_back(keys, values, query_stack, cot_stack, log_row, mask, scale):
    scores = dot_nt(keys, query_stack) * scale
    weights = jnp.where(mask, jnp.exp(scores - log_row), 0.0)
    weights_low = weights.astype(BF16)
    grad_prob = dot_nt(values, cot_stack)
    delta = jnp.sum(weights_low.astype(F32) * grad_prob, axis=0, keepdims=True)
    dscore = (weights * (grad_prob - delta)).astype(BF16)
    dquery = dot_nn(keys.T, dscore)
    return dquery, dot_nn(dscore, query_stack) * scale, dot_nn(weights_low, cot_stack)


def grid_of(count):
    width = 1
    while width * width * 4 <= count:
        width *= 2
    while count % width:
        width //= 2
    return count // width, width


def meet(peers):
    barrier = pltpu.get_barrier_semaphore()
    for peer in peers:
        pl.semaphore_signal(barrier, inc=1, device_id=peer, device_id_type=MESH)
    pl.semaphore_wait(barrier, len(peers))


def step_kernel(
    kv_count, tp_count, group, scale,
    lists_ref, spots_ref, slots_ref, own_ref,
    wanted_ref, k_ref, v_ref, gate_ref, log_ref, hidden_ref, q_hbm, g_hbm,
    dq_ref, gw_ref, kept_ref, got_ref, pool_got, asked_ref, hid_all,
    q_buf, g_buf, kv_all, kv_own, kv_in, kv_out, want_in, want,
    pooled, pool_acc, pool_out, dq_pool, dq_far,
    parts, out_box, turned, tile, z_out, z_in,
    in_sem, z_send, z_recv, y_send, y_recv, t_send, t_recv,
    p_send, p_recv, w_send, w_recv, pg_send, pg_recv,
    hy_send, hy_recv, hx_send, hx_recv, hs_send, hs_recv, dq_send, dq_recv,
    a_send, a_recv, s_send, s_recv,
):
    nz, ny = grid_of(kv_count)
    me = lax.axis_index("kv")
    tp = lax.axis_index("tp")
    z = me // ny
    y = lax.rem(me, ny)
    cores = 2 if tp_count % 2 == 0 else 1
    nx = tp_count // cores
    x = tp // cores
    core = lax.rem(tp, cores)
    blocks_here = k_ref.shape[0]
    tokens = blocks_here * KEY_BLOCK
    heads = k_ref.shape[2] // HEAD_DIM
    steps = tokens // QUERY_BLOCK
    requests = steps * CHOSEN
    pool_count = pooled.shape[0] * pooled.shape[1]
    pool_here = pooled.shape[1]
    hidden_rows = hidden_ref.shape[0]
    rows, cols = gw_ref.shape
    head_cols = group * HEAD_DIM
    wide = 2 * HEAD_DIM
    width = group * QUERY_BLOCK
    box = CAP * KEY_BLOCK
    own_keys = (k_ref, v_ref)
    for h in range(heads):
        for p in range(2):
            kv_own[h, p] = own_keys[p][:, :, h * HEAD_DIM : (h + 1) * HEAD_DIM]
    meet(
        [{"kv": lax.rem(me + d, kv_count)} for d in range(1, kv_count)]
        + [{"tp": lax.rem(tp + d, tp_count)} for d in range(1, tp_count)]
    )

    def remote(src, dst, send, recv, to):
        return pltpu.make_async_remote_copy(
            src_ref=src, dst_ref=dst, send_sem=send, recv_sem=recv,
            device_id=to, device_id_type=MESH,
        )

    def source(h, side, s):
        return kv_own.at[h] if s == 0 else kv_in[h][side][s - 1]

    def z_copy(h, side, s):
        to = z + 1 if side == 0 else z - 1
        return remote(
            source(h, side, s), kv_in[h][side][s],
            z_send.at[h, side, s], z_recv.at[h, side, s], {"kv": to * ny + y},
        )

    def y_copy(h, row, d):
        at = nz * blocks_here + (row * (ny - 1) + d - 1) * CAP
        return remote(
            kv_out.at[h, row, d - 1], kv_all[h].at[:, pl.ds(at, CAP)],
            y_send.at[h, row, d - 1], y_recv.at[h, row, d - 1],
            {"kv": z * ny + lax.rem(y + d, ny)},
        )

    def t_copy(d):
        return remote(
            wanted_ref, want_in.at[d - 1], t_send.at[d - 1], t_recv.at[d - 1],
            {"kv": z * ny + lax.rem(y + d, ny)},
        )

    def there(side, s):
        return z >= s if side == 0 else z + s < nz

    def onward(side):
        return z < nz - 1 if side == 0 else z > 0

    def pass_z(h, side, s):
        if s < nz - 1:
            @pl.when(onward(side))
            def _():
                z_copy(h, side, s).start()

    def pass_y(h, side, s):
        row = z - s if side == 0 else z + s
        held = source(h, side, s)
        kv_all[h][:, pl.ds(row * blocks_here, blocks_here)] = held[...]
        for d in range(1, ny):
            for c in range(CAP):
                block = want[ny - d - 1, row * ny + y, 0, h * CAP + c]
                for p in range(2):
                    kv_out[h, row, d - 1, p, c] = held[p, block]
            y_copy(h, row, d).start()

    def relay_keys(h, s):
        if h >= heads:
            return
        for side in range(2):
            @pl.when(there(side, s))
            def _():
                z_copy(h, side, s - 1).wait_recv()
                pass_z(h, side, s)

        for side in range(2):
            @pl.when(there(side, s))
            def _():
                pass_y(h, side, s)

    def keys_complete(h):
        for row in range(nz):
            for d in range(1, ny):
                y_copy(h, row, d).wait_recv()

    def others(make):
        return [make(d) for d in range(1, kv_count)]

    def spread(src, dst, send, recv):
        def make(d):
            to = lax.rem(me + d, kv_count)
            return remote(src(to), dst.at[me], send.at[d - 1], recv.at[d - 1], {"kv": to})

        return others(make)

    fetches = [
        pltpu.make_async_copy(q_hbm, q_buf, in_sem.at[0]),
        pltpu.make_async_copy(g_hbm, g_buf, in_sem.at[1]),
        pltpu.make_async_copy(wanted_ref.at[me], asked_ref.at[me], in_sem.at[2]),
    ]
    def hid_piece(row):
        return tile.at[row * hidden_rows : (row + 1) * hidden_rows]

    hid_local = [
        pltpu.make_async_copy(
            hidden_ref.at[:, pl.ds(pl.multiple_of((row * ny + y) * rows, rows), rows)],
            hid_piece(row),
            in_sem.at[3 + row],
        )
        for row in range(nz)
    ]
    hid_home = [
        pltpu.make_async_copy(
            hid_piece(row),
            hid_all.at[row, pl.ds(pl.multiple_of((y * tp_count + tp) * hidden_rows, hidden_rows), hidden_rows)],
            in_sem.at[3 + row],
        )
        for row in range(nz)
    ]

    def hid_rows(col, part):
        at = (col * tp_count + part) * hidden_rows
        return hid_all.at[:, pl.ds(pl.multiple_of(at, hidden_rows), hidden_rows)]

    def hy_copy(d, row):
        to = lax.rem(y + d, ny)
        return remote(
            hidden_ref.at[:, pl.ds(pl.multiple_of((row * ny + to) * rows, rows), rows)],
            hid_all.at[row, pl.ds(pl.multiple_of((y * tp_count + tp) * hidden_rows, hidden_rows), hidden_rows)],
            hy_send.at[d - 1, row], hy_recv.at[d - 1, row], {"kv": z * ny + to},
        )

    def hx_copy(e, d):
        col = lax.rem(y + ny - e, ny)
        to = lax.rem(x + d, nx) * cores + core
        return remote(
            hid_rows(col, tp), hid_rows(col, tp),
            hx_send.at[e, d - 1], hx_recv.at[e, d - 1], {"tp": to},
        )

    def hs_copy(e, d):
        col = lax.rem(y + ny - e, ny)
        part = lax.rem(x + nx - d, nx) * cores + core
        return remote(
            hid_rows(col, part), hid_rows(col, part),
            hs_send.at[e, d], hs_recv.at[e, d], {"tp": x * cores + 1 - core},
        )

    def hidden_out(e):
        for d in range(1, nx):
            hx_copy(e, d).start()
        if cores > 1:
            hs_copy(e, 0).start()

    def hidden_on(e):
        for d in range(1, nx):
            hx_copy(e, d).wait_recv()
            if cores > 1:
                hs_copy(e, d).start()

    def exchange(h, dz, dy):
        to = lax.rem(z + dz, nz) * ny + lax.rem(y + dy, ny)
        n = dz * ny + dy
        return remote(
            out_box.at[h, to],
            got_ref.at[h, pl.ds(pl.multiple_of(me * box, box), box)],
            a_send.at[h, n], a_recv.at[h, n], {"kv": to},
        )

    def dq_copy(h, d):
        return remote(
            dq_ref.at[:, h * head_cols : (h + 1) * head_cols], dq_far.at[h, d - 1],
            dq_send.at[h, d - 1], dq_recv.at[h, d - 1],
            {"kv": z * ny + lax.rem(y + d, ny)},
        )

    right = nz - 1 - z
    right_first = z * 2 < nz

    def owner_row(i):
        ahead = jnp.where(i < right, nz - 1 - i, i - right)
        back = jnp.where(i < z, i, nz - 1 - (i - z))
        return jnp.where(right_first, ahead, back)

    def goes_right(i):
        return jnp.where(right_first, jnp.where(i < right, 1, 0), jnp.where(i < z, 0, 1)) > 0

    def sum_copy(h, i):
        to = jnp.where(goes_right(i), z + 1, z - 1)
        slot = jnp.where(goes_right(i), owner_row(i) - to, nz - to + owner_row(i))
        return remote(
            z_out.at[h, i], z_in.at[h, slot], s_send.at[h, i], s_recv.at[h, slot],
            {"kv": to * ny + y},
        )

    def sum_came(h, slot):
        return remote(
            z_out.at[h, 0], z_in.at[h, slot], s_send.at[h, 0], s_recv.at[h, slot],
            {"kv": lax.rem(me + ny, kv_count)},
        )

    def in_slot(i):
        return jnp.where(goes_right(i), owner_row(i) - z, nz - z + owner_row(i))

    def has_in(i):
        return jnp.where(goes_right(i), jnp.where(z > 0, 1, 0), jnp.where(z < nz - 1, 1, 0)) > 0

    pass_z(0, 0, 0)
    pass_z(0, 1, 0)
    for d in range(1, ny):
        t_copy(d).start()
    pick = (
        lax.broadcasted_iota(jnp.int32, (pool_here, tokens), 1) // POOL_BLOCK
        == lax.broadcasted_iota(jnp.int32, (pool_here, tokens), 0)
    ).astype(BF16)
    for p in range(2):
        all_rows = own_keys[p][...].reshape(tokens, heads * HEAD_DIM)
        mean = (dot_nn(pick, all_rows) / POOL_BLOCK).astype(BF16)
        pooled[me, :, p * heads * HEAD_DIM : (p + 1) * heads * HEAD_DIM] = mean
    pool_sends = spread(lambda to: pooled.at[me], pooled, p_send, p_recv)
    for copy in pool_sends:
        copy.start()
    want_sends = spread(lambda to: wanted_ref.at[to], asked_ref, w_send, w_recv)
    for copy in fetches + hid_local + want_sends:
        copy.start()
    parts[requests] = jnp.zeros((KEY_BLOCK, wide), BF16)
    pool_acc[...] = jnp.zeros_like(pool_acc)
    for there_copy, home_copy in zip(hid_local, hid_home):
        there_copy.wait()
        home_copy.start()
    for copy in hid_home:
        copy.wait()
    hidden_out(0)
    for d in range(1, ny):
        t_copy(d).wait_recv()
    for copy in fetches:
        copy.wait()
    to_scalar = pltpu.make_async_copy(want_in, want, in_sem.at[0])
    to_scalar.start()
    to_scalar.wait()
    pass_y(0, 0, 0)

    def hy_start(row):
        if row < nz:
            for d in range(1, ny):
                hy_copy(d, row).start()

    hy_start(0)
    for copy in pool_sends:
        copy.wait_recv()

    def load_step(h, b, branch):
        at = pl.ds(pl.multiple_of(b * QUERY_BLOCK, QUERY_BLOCK), QUERY_BLOCK)
        first = h * head_cols
        stack = jnp.concatenate(
            [q_buf[at, first + r * HEAD_DIM : first + (r + 1) * HEAD_DIM] for r in range(group)],
            axis=0,
        )
        gates = gate_ref[branch, :, at].T
        cots = jnp.concatenate(
            [
                (
                    gates[:, h * group + r : h * group + r + 1]
                    * g_buf[at, first + r * HEAD_DIM : first + (r + 1) * HEAD_DIM].astype(F32)
                ).astype(BF16)
                for r in range(group)
            ],
            axis=0,
        )
        logs = log_ref[branch, :, at]
        log_row = jnp.concatenate(
            [logs[h * group + r : h * group + r + 1, :] for r in range(group)], axis=1
        )
        query_pos = (
            me * tokens + b * QUERY_BLOCK
            + lax.broadcasted_iota(jnp.int32, (1, width), 1) % QUERY_BLOCK
        )
        return at, stack, cots, log_row, query_pos

    def pool_steps(h, low, high):
        def one(b, carry):
            at, stack, cots, log_row, query_pos = load_step(h, b, 0)
            pool_end = (
                lax.broadcasted_iota(jnp.int32, (pool_count, width), 0) * POOL_BLOCK
                + POOL_BLOCK - 1
            )
            first = h * HEAD_DIM
            keys = pooled[:, :, first : first + HEAD_DIM].reshape(pool_count, HEAD_DIM)
            first += heads * HEAD_DIM
            values = pooled[:, :, first : first + HEAD_DIM].reshape(pool_count, HEAD_DIM)
            dq, dk, dv = branch_back(
                keys, values, stack, cots, log_row, pool_end <= query_pos, scale
            )
            dq_pool[h * steps + b] = dq
            pool_acc[h] += jnp.concatenate([dk, dv], axis=1)
            return carry

        lax.fori_loop(low, high, one, 0)

    def pick_steps(h, low, high):
        def one(b, carry):
            at, stack, cots, log_row, query_pos = load_step(h, b, 1)
            ids = [lists_ref[h, b * CHOSEN + c] for c in range(CHOSEN)]
            spots = [spots_ref[h, b * CHOSEN + c] for c in range(CHOSEN)]
            keys = jnp.concatenate([kv_all[h][0, i] for i in spots], axis=0)
            values = jnp.concatenate([kv_all[h][1, i] for i in spots], axis=0)
            offset = lax.broadcasted_iota(jnp.int32, (KEY_BLOCK, width), 0)
            key_pos = jnp.concatenate([offset + i * KEY_BLOCK for i in ids], axis=0)
            dq, dk, dv = branch_back(
                keys, values, stack, cots, log_row, key_pos <= query_pos, scale
            )
            parts[pl.ds(b * CHOSEN, CHOSEN)] = (
                jnp.concatenate([dk, dv], axis=1).astype(BF16).reshape(CHOSEN, KEY_BLOCK, wide)
            )
            dq = (dq + dq_pool[h * steps + b]) * scale
            for r in range(group):
                first = h * head_cols + r * HEAD_DIM
                dq_ref[at, first : first + HEAD_DIM] = dq[
                    :, r * QUERY_BLOCK : (r + 1) * QUERY_BLOCK
                ].T.astype(BF16)
            return carry

        lax.fori_loop(low, high, one, 0)

    def pack(h):
        def to_owner(d, carry):
            owner = lax.rem(me + d, kv_count)
            for c in range(CAP):
                out_box[h, owner, c * KEY_BLOCK : (c + 1) * KEY_BLOCK, :] = parts[
                    slots_ref[h, owner * CAP + c]
                ]
            return carry

        lax.fori_loop(1, kv_count, to_owner, 0)

    def keep(h):
        def to_self(b, carry):
            total = parts[own_ref[h, b * steps]].astype(F32)
            for step in range(1, steps):
                total += parts[own_ref[h, b * steps + step]].astype(F32)
            at = pl.ds(pl.multiple_of(b * KEY_BLOCK, KEY_BLOCK), KEY_BLOCK)
            kept_ref[at, h * wide : (h + 1) * wide] = total
            return carry

        lax.fori_loop(0, blocks_here, to_self, 0)

    def send_boxes(h, near):
        for dy in range(1) if near else range(1, ny):
            for dz in range(1 if dy == 0 else 0, nz):
                exchange(h, dz, dy).start()

    def weigh(h, i):
        lane = min(256, head_cols)

        def one(c, carry):
            at = pl.ds(pl.multiple_of(c * lane, lane), lane)
            from_self = pl.ds(pl.multiple_of(h * head_cols + c * lane, lane), lane)
            total = dot_nn(turned[i, 0], dq_ref[:, from_self])
            for d in range(1, ny):
                total += dot_nn(turned[i, d], dq_far[h, d - 1, :, at])
            if i < nz - 1:
                z_out[h, i, :, at] = total.astype(BF16)
            else:
                gw_ref[:, from_self] = total
            return carry

        lax.fori_loop(0, head_cols // lane, one, 0)

    def sum_first(h):
        for d in range(1, ny):
            dq_copy(h, d).wait_recv()
        for i in range(nz):
            weigh(h, i)
            if i < nz - 1:
                @pl.when(jnp.logical_not(has_in(i)))
                def _():
                    sum_copy(h, i).start()

    def sum_relay(h, i):
        @pl.when(has_in(i))
        def _():
            sum_came(h, in_slot(i)).wait_recv()
            z_out[h, i] = (
                z_out[h, i].astype(F32) + z_in[h, in_slot(i)].astype(F32)
            ).astype(BF16)
            sum_copy(h, i).start()

    def sum_last(h):
        at = slice(h * head_cols, (h + 1) * head_cols)
        for slot, some in ((0, z > 0), (nz, z < nz - 1)):
            @pl.when(some)
            def _():
                sum_came(h, slot).wait_recv()
                gw_ref[:, at] += z_in[h, slot].astype(F32)

    half = max(steps * 3 // 4, 1)
    pool_steps(0, 0, half)
    relay_keys(0, 1)
    hy_start(1)
    pool_steps(0, half, steps)
    for h in range(1, heads):
        pool_steps(h, 0, steps)
    for s in range(2, nz):
        relay_keys(0, s)
        hy_start(s)
        if s == 2 and heads > 1:
            pass_z(1, 0, 0)
            pass_z(1, 1, 0)
            pass_y(1, 0, 0)
    for h in range(heads):
        pool_out[:, :, h * wide : (h + 1) * wide] = (
            pool_acc[h].astype(BF16).reshape(kv_count, pool_here, wide)
        )
    pool_grads = spread(lambda to: pool_out.at[to], pool_got, pg_send, pg_recv)
    for copy in pool_grads:
        copy.start()
    own_pool = pltpu.make_async_copy(pool_out.at[me], pool_got.at[me], in_sem.at[0])
    own_pool.start()
    hidden_on(0)

    def hidden_arrived():
        for d in range(1, ny):
            for row in range(nz):
                hy_copy(d, row).wait_recv()
            hidden_out(d)

    def hidden_ready(e):
        if e > 0:
            hidden_on(e)
        if cores > 1:
            for d in range(nx):
                hs_copy(e, d).wait_recv()
        col = lax.rem(y + ny - e, ny)
        at = pl.ds(pl.multiple_of(col * tokens, tokens), tokens)
        for i in range(nz):
            grab = pltpu.make_async_copy(hid_all.at[owner_row(i), at], tile, in_sem.at[1])
            grab.start()
            grab.wait()
            turned[i, e] = tile[...].T

    hidden_ready(0)
    for h in range(heads):
        keys_complete(h)
        cuts = [max(steps // 4, 1), max(steps // 2, 1), steps * 7 // 8, steps]
        low = 0
        for i, high in enumerate(cuts):
            pick_steps(h, low, high)
            low = high
            if h > 0:
                for j in range(nz - 1):
                    if min(j, 2) == i:
                        sum_relay(h - 1, j)
            if i == 0:
                relay_keys(h + 1, 1)
                if h == 0:
                    hidden_arrived()
            if i == 2:
                relay_keys(h + 1, 2)
        for d in range(1, ny):
            dq_copy(h, d).start()
        pack(h)
        send_boxes(h, True)
        for s in range(3, nz):
            relay_keys(h + 1, s)
        if h + 2 < heads:
            pass_z(h + 2, 0, 0)
            pass_z(h + 2, 1, 0)
            pass_y(h + 2, 0, 0)
        send_boxes(h, False)
        keep(h)
        if h == 0:
            for e in range(1, ny):
                hidden_ready(e)
        sum_first(h)
    for i in range(nz - 1):
        sum_relay(heads - 1, i)
    for h in range(heads):
        sum_last(h)

    own_pool.wait()
    for copy in pool_sends:
        copy.wait_send()
    for copy in want_sends + pool_grads:
        copy.wait()
    for d in range(1, ny):
        t_copy(d).wait_send()
    for h in range(heads):
        for s in range(nz - 1):
            for side in range(2):
                @pl.when(there(side, s))
                def _():
                    @pl.when(onward(side))
                    def _():
                        z_copy(h, side, s).wait_send()

        for row in range(nz):
            for d in range(1, ny):
                y_copy(h, row, d).wait_send()
        for d in range(1, ny):
            dq_copy(h, d).wait_send()
        for dz in range(nz):
            for dy in range(ny):
                if dz or dy:
                    exchange(h, dz, dy).wait()
        for i in range(nz - 1):
            sum_copy(h, i).wait_send()
    for d in range(1, ny):
        for row in range(nz):
            hy_copy(d, row).wait_send()
    for e in range(ny):
        for d in range(1, nx):
            hx_copy(e, d).wait_send()
        if cores > 1:
            for d in range(nx):
                hs_copy(e, d).wait_send()


def settle_kernel(
    kv_count, place_ref, asked_ref, got_ref, pool_ref, kept_ref, gk_ref, gv_ref, acc
):
    head = pl.program_id(0)
    tokens = kept_ref.shape[0]
    pool_here = tokens // POOL_BLOCK
    box = CAP * KEY_BLOCK
    pooled = sum(pool_ref[i].astype(F32) for i in range(kv_count)) / POOL_BLOCK
    for j in range(pool_here):
        rows = slice(j * POOL_BLOCK, (j + 1) * POOL_BLOCK)
        acc[rows, :] = kept_ref[rows, :] + pooled[j : j + 1, :]

    def source(i, carry):
        other = lax.rem(place_ref[0] + 1 + i, kv_count)
        for c in range(CAP):
            block = asked_ref[other, head * CAP + c]
            rows = pl.ds(pl.multiple_of(block * KEY_BLOCK, KEY_BLOCK), KEY_BLOCK)
            came = pl.ds(pl.multiple_of(other * box + c * KEY_BLOCK, KEY_BLOCK), KEY_BLOCK)
            acc[rows, :] += got_ref[0, came, :].astype(F32)
        return carry

    lax.fori_loop(0, kv_count - 1, source, 0)
    gk_ref[...] = acc[:, :HEAD_DIM].astype(BF16)
    gv_ref[...] = acc[:, HEAD_DIM:].astype(BF16)


def body(hidden_rows, queries, key_rows, value_rows, branch_gates, log_sums, chosen, out_grad):
    kv_count = lax.axis_size("kv")
    tp_count = lax.axis_size("tp")
    kv_index = lax.axis_index("kv")
    tokens = queries.shape[0]
    kv_local = key_rows.shape[1] // HEAD_DIM
    group = HEADS // KV_HEADS
    scale = HEAD_DIM ** (-0.5)
    seq_len = tokens * kv_count
    steps = tokens // QUERY_BLOCK
    blocks_here = tokens // KEY_BLOCK
    pool_here = tokens // POOL_BLOCK
    request_count = steps * CHOSEN
    slot_count = kv_count * CAP
    nz, ny = grid_of(kv_count)

    lists = chosen.reshape(kv_local, request_count)
    owners = lists // blocks_here
    local_block = lists % blocks_here
    remote = owners != kv_index
    order = jnp.arange(request_count, dtype=jnp.int32)
    rank_in = jnp.sum(
        (
            (owners[:, :, None] == owners[:, None, :]) & (order[None, None, :] < order[None, :, None])
        ).astype(jnp.int32),
        axis=-1,
    )
    slot_index = jnp.where(remote, owners * CAP + rank_in, slot_count)
    hit = slot_index[:, None, :] == jnp.arange(slot_count, dtype=jnp.int32)[None, :, None]
    slot_from = request_count + jnp.sum(jnp.where(hit, order - request_count, 0), axis=-1)
    wanted = jnp.sum(jnp.where(hit, local_block[:, None, :], 0), axis=-1)
    wanted = (
        wanted.reshape(kv_local, kv_count, CAP).transpose(1, 0, 2).reshape(kv_count, 1, -1)
    )
    wanted = jnp.pad(wanted, ((0, 0), (0, 0), (0, 128 - kv_local * CAP)))
    own_block = jnp.where(remote, -1, local_block).reshape(kv_local, 1, steps, CHOSEN)
    same = own_block == jnp.arange(blocks_here, dtype=jnp.int32)[None, :, None, None]
    own_from = (
        request_count
        + jnp.sum(jnp.where(same, order.reshape(steps, CHOSEN) - request_count, 0), axis=-1)
    ).reshape(kv_local, blocks_here * steps)
    place = kv_index.astype(jnp.int32).reshape(1)
    row, col = owners // ny, owners % ny
    here = kv_index % ny
    away = (here - col + ny) % ny
    spots = jnp.where(
        away == 0,
        row * blocks_here + local_block,
        nz * blocks_here + (row * (ny - 1) + away - 1) * CAP + rank_in,
    )

    wide = 2 * HEAD_DIM
    box = CAP * KEY_BLOCK
    model = hidden_rows.shape[1]
    out_rows = model // kv_count
    head_cols = group * HEAD_DIM
    out_cols = kv_local * head_cols
    far = max(ny - 1, 1)
    cores = 2 if tp_count % 2 == 0 else 1
    nx = tp_count // cores
    side = max(nx - 1, 1)
    dma = pltpu.SemaphoreType.DMA
    anywhere = pl.BlockSpec(memory_space=pl.ANY)
    inside = pl.BlockSpec(memory_space=pltpu.VMEM)
    scalars = pl.BlockSpec(memory_space=pltpu.SMEM)
    vmem = pltpu.VMEM
    out = jax.ShapeDtypeStruct
    grad_queries, grad_weight, kept, got, pool_got, asked, _ = pl.pallas_call(
        functools.partial(step_kernel, kv_count, tp_count, group, scale),
        in_specs=[scalars] * 4 + [inside] * 5 + [anywhere] * 3,
        out_specs=[inside, inside, inside, anywhere, anywhere, inside, anywhere],
        out_shape=[
            out((tokens, out_cols), BF16),
            out((out_rows, out_cols), F32),
            out((tokens, kv_local * wide), F32),
            out((kv_local, kv_count * box, wide), BF16),
            out((kv_count, pool_here, kv_local * wide), BF16),
            out((kv_count, 1, 128), jnp.int32),
            out((nz, ny * tokens, out_rows), BF16),
        ],
        scratch_shapes=[
            vmem((tokens, out_cols), BF16),
            vmem((tokens, out_cols), BF16),
            [
                vmem((2, nz * (blocks_here + (ny - 1) * CAP), KEY_BLOCK, HEAD_DIM), BF16)
                for _ in range(kv_local)
            ],
            vmem((kv_local, 2, blocks_here, KEY_BLOCK, HEAD_DIM), BF16),
            [
                [
                    [vmem((2, blocks_here, KEY_BLOCK, HEAD_DIM), BF16) for _ in range(nz - 1)]
                    for _ in range(2)
                ]
                for _ in range(kv_local)
            ],
            vmem((kv_local, nz, far, 2, CAP, KEY_BLOCK, HEAD_DIM), BF16),
            vmem((far, kv_count, 1, 128), jnp.int32),
            pltpu.SMEM((far, kv_count, 1, 128), jnp.int32),
            vmem((kv_count, pool_here, kv_local * wide), BF16),
            vmem((kv_local, kv_count * pool_here, wide), F32),
            vmem((kv_count, pool_here, kv_local * wide), BF16),
            vmem((kv_local * steps, HEAD_DIM, group * QUERY_BLOCK), F32),
            vmem((kv_local, far, tokens, head_cols), BF16),
            vmem((request_count + 1, KEY_BLOCK, wide), BF16),
            vmem((kv_local, kv_count, box, wide), BF16),
            vmem((nz, ny, out_rows, tokens), BF16),
            vmem((tokens, out_rows), BF16),
            vmem((kv_local, max(nz - 1, 1), out_rows, head_cols), BF16),
            vmem((kv_local, nz + 1, out_rows, head_cols), BF16),
            dma((3 + nz,)),
            dma((kv_local, 2, nz)), dma((kv_local, 2, nz)),
            dma((kv_local, nz, far)), dma((kv_local, nz, far)), dma((far,)), dma((far,)),
            dma((kv_count,)), dma((kv_count,)), dma((kv_count,)), dma((kv_count,)),
            dma((kv_count,)), dma((kv_count,)),
            dma((far, nz)), dma((far, nz)), dma((ny, side)), dma((ny, side)),
            dma((ny, nx)), dma((ny, nx)), dma((kv_local, far)), dma((kv_local, far)),
            dma((kv_local, kv_count)), dma((kv_local, kv_count)),
            dma((kv_local, nz)), dma((kv_local, nz + 1)),
        ],
        compiler_params=pltpu.CompilerParams(
            collective_id=0, has_side_effects=True, vmem_limit_bytes=VMEM_LIMIT
        ),
        name="step",
    )(
        lists, spots, slot_from, own_from,
        wanted,
        key_rows.reshape(blocks_here, KEY_BLOCK, kv_local * HEAD_DIM),
        value_rows.reshape(blocks_here, KEY_BLOCK, kv_local * HEAD_DIM),
        branch_gates, log_sums, hidden_rows, queries, out_grad,
    )

    grad_keys, grad_values = pl.pallas_call(
        functools.partial(settle_kernel, kv_count),
        grid_spec=pltpu.PrefetchScalarGridSpec(
            num_scalar_prefetch=2,
            grid=(kv_local,),
            in_specs=[
                pl.BlockSpec((1, kv_count * box, wide), lambda h, *_: (h, 0, 0)),
                pl.BlockSpec((kv_count, pool_here, wide), lambda h, *_: (0, 0, h)),
                pl.BlockSpec((tokens, wide), lambda h, *_: (0, h)),
            ],
            out_specs=[
                pl.BlockSpec((tokens, HEAD_DIM), lambda h, *_: (0, h)),
                pl.BlockSpec((tokens, HEAD_DIM), lambda h, *_: (0, h)),
            ],
            scratch_shapes=[pltpu.VMEM((tokens, wide), F32)],
        ),
        out_shape=[
            jax.ShapeDtypeStruct((tokens, kv_local * HEAD_DIM), BF16),
            jax.ShapeDtypeStruct((tokens, kv_local * HEAD_DIM), BF16),
        ],
        cost_estimate=pl.CostEstimate(
            flops=4 * 2**20, bytes_accessed=8 * 2**20, transcendentals=0
        ),
        name="settle",
    )(place, asked.reshape(kv_count, 128), got, pool_got, kept)
    return (grad_queries, grad_keys, grad_values, grad_weight)


def solution(mesh):
    placed = (
        P(("kv", "tp"), None),
        P("kv", "tp"),
        P("kv", "tp"),
        P("kv", "tp"),
        P(None, "tp", "kv"),
        P(None, "tp", "kv"),
        P("tp", "kv", None),
        P("kv", "tp"),
    )
    return jax.shard_map(
        body,
        mesh=mesh,
        in_specs=placed,
        out_specs=(P("kv", "tp"), P("kv", "tp"), P("kv", "tp"), P("kv", "tp")),
        check_vma=False,
    )
```
